512 devices in a mesh: sp: 32 (over z, x), tp: 16 (over y, core).
Axes of the slice: x: 4, y: 8, z: 8, core: 2. Of those that a mesh axis runs over, the one named last changes fastest.
Arguments:
- moe_input: bfloat16 [6144, 2048], P('sp'), may hold values from -6 to 6
- out_grad: bfloat16 [6144, 2048], P('sp', 'tp'), may hold values from -6 to 6
- expert_ids: int32 [6144, 2], P('sp'), may hold values from 0 to 31, all different within a row; in each aligned block of 192 rows (0 to 191, 192 to 383, ...) at most 15 rows name the same one
- expert_weights: float32 [6144, 2], P('sp'), may hold values from 0.1 to 0.9
- w_gate: bfloat16 [32, 2048, 2048], P('sp', None, 'tp'), may hold values from -0.125 to 0.125
- w_up: bfloat16 [32, 2048, 2048], P('sp', None, 'tp'), may hold values from -0.125 to 0.125
- w_down: bfloat16 [32, 2048, 2048], P('sp', 'tp'), may hold values from -0.125 to 0.125
- out_proj: bfloat16 [1536, 2048], P('tp'), may hold values from -0.15625 to 0.15625
- retained: bfloat16 [6144, 1536], P('sp', 'tp'), may hold values from -6 to 6
- queries: bfloat16 [6144, 768], P('sp', 'tp'), may hold values from -6 to 6
- keys: bfloat16 [6144, 768], P('sp', 'tp'), may hold values from -0.86328125 to 0.86328125
- values: bfloat16 [6144, 1536], P('sp', 'tp'), may hold values from -6 to 6
- log_decay: float32 [6144, 16], P('sp', 'tp'), may hold values from -1 to 0
- incoming_state: float32 [32, 16, 48, 96], P('sp', 'tp'), may hold values from -6 to 6
Outputs:
- w_gate_grad: bfloat16 [32, 2048, 2048], P('sp', None, 'tp')
- w_up_grad: bfloat16 [32, 2048, 2048], P('sp', None, 'tp')
- w_down_grad: bfloat16 [32, 2048, 2048], P('sp', 'tp')
- out_proj_grad: float32 [2048, 1536], P('sp', 'tp')
- query_grad: bfloat16 [6144, 768], P('sp', 'tp')
- key_grad: bfloat16 [6144, 768], P('sp', 'tp')
- value_grad: bfloat16 [6144, 1536], P('sp', 'tp')
The draws below stay inside these ranges and needn't reach their ends.
Inputs may be any that keep to these rules, and one draw needn't show every extreme that they name: `expert_ids`: in each aligned block of 192 positions no expert is named by more than 15 of the block's assignments, a bound that some block reaches.
All inputs are finite; a program needn't handle non-finite values.
Results may differ from the reference program's by a relative error of at most 0.02.
Values may be sent and summed in bfloat16 or wider, within the bound.
No kernel may reach another device: no remote copies, remote signals or barrier semaphores. Data moves between devices by JAX's collectives and lax.ppermute only.
A program may use at most 64 MiB of HBM per device.

```python
import math
import jax
import jax.numpy as jnp
import numpy as np
from jax import lax

D = 2048
RETENTION_HEADS = 16
KEY_DIM = 48
VALUE_DIM = 96
FF = 2048
TOK_DEV = 192
SEQUENCE_TOKENS = 6144
EXPERTS = 32
CAP = 15
RET_WIDTH = 1536
KEY_WIDTH = 768
N_SP = 32
N_TP = 16


def draw_log_decay(key, part):
    keys = jax.random.split(jax.random.fold_in(key, 17), 7)
    slow_share = 0.5
    slow = jax.random.uniform(keys[0], (RETENTION_HEADS,), jnp.float32) < slow_share
    slow_rate = jnp.exp(jax.random.uniform(keys[1], (RETENTION_HEADS,), jnp.float32, jnp.log(0.1), jnp.log(0.6))) / SEQUENCE_TOKENS
    fast_rate = jax.random.uniform(keys[2], (RETENTION_HEADS,), jnp.float32, 1.0 / 50.0, 1.0 / 30.0)
    decay_rate = jnp.where(slow, slow_rate, fast_rate)
    block_multiplier = jnp.repeat(jax.random.uniform(keys[3], (SEQUENCE_TOKENS // TOK_DEV,), jnp.float32, 0.5, 1.6), TOK_DEV)
    coarse_estimate = jax.random.uniform(keys[4], (SEQUENCE_TOKENS, 1), jnp.float32, 0.5, 1.5)
    spike_position = jax.random.randint(keys[5], (3,), 0, SEQUENCE_TOKENS)
    spike_mask = jnp.any(jnp.arange(SEQUENCE_TOKENS)[:, None] == spike_position[None, :], axis=1).astype(jnp.float32)
    spike_length = jax.random.uniform(keys[6], (RETENTION_HEADS,), jnp.float32, 0.22, 0.51)
    return -(decay_rate[None, :] * block_multiplier[:, None] * coarse_estimate) - spike_mask[:, None] * spike_length[None, :]


def raised(drawn, rng, source, target, blocks, factor):
    owner, partner = [(jnp.arange(drawn.shape[axis_at]) // (drawn.shape[axis_at] // blocks)).reshape([-1 if axis == axis_at else 1 for axis in range(drawn.ndim)]) for axis_at in (source, target)]
    chosen = jax.random.permutation(rng, blocks)[partner]
    strong = (owner == chosen) | (owner == (partner + blocks // 2) % blocks)
    return jnp.where(strong, factor * drawn, drawn)


def block_scale(key, shape, pieces, smallest, high):
    def one(position, blocks):
        heights = jax.random.uniform(jax.random.fold_in(jax.random.fold_in(key, 6), position), (blocks,), jnp.float32, smallest / len(pieces), high / len(pieces))
        return jnp.repeat(jnp.exp(heights), shape[position] // blocks).reshape((-1,) + (1,) * (len(shape) - position - 1))

    gain = one(*pieces[0])
    for cut in pieces[1:]:
        gain = gain * one(*cut)
    return gain


def deal_out(rng, own, number, rows, number_of, top, bound, slope):
    sequence = jax.random.permutation(rng, number_of)
    crowded, usual = load_shares(number_of, rows * top, bound, slope, True), load_shares(number_of, rows * top, bound, slope, False)
    places = jnp.arange(number_of)

    def named(tallies, rotation):
        used = int((tallies > 0).sum())
        fixed = max(1, used // 4)
        moved = fixed + (places - fixed + rotation * (used - fixed)) % max(1, number_of - fixed)
        return jnp.zeros((number_of,), jnp.int32).at[sequence[jnp.where(places < fixed, places, moved)]].set(jnp.asarray(tallies, jnp.int32))

    tallies = jnp.where(number % 4 == 0, named(crowded, number // 4), named(usual, number - number // 4 - 1))
    mixed = jax.random.permutation(jax.random.fold_in(own, 3), number_of)
    giver, receiver = mixed[0:number_of // 2 * 2:2], mixed[1:number_of // 2 * 2:2]
    slack = jnp.minimum(tallies[giver] - 1, bound - tallies[receiver]) // 2
    slack = jnp.where((giver == sequence[0]) | (receiver == sequence[0]) | (tallies[receiver] == 0), 0, jnp.maximum(slack, 0))
    moved = jax.random.randint(jax.random.fold_in(own, 4), (number_of // 2,), 0, 1 << 20) % (slack + 1)
    tallies = tallies.at[giver].add(-moved).at[receiver].add(moved)
    items = jnp.searchsorted(jnp.cumsum(tallies), jnp.arange(rows * top), side="right").astype(jnp.int32)
    grid = items.reshape(top, rows).T
    grid = grid[jax.random.permutation(jax.random.fold_in(own, 1), rows)]
    rotation = jax.random.randint(jax.random.fold_in(own, 2), (rows, 1), 0, top)
    return jnp.take_along_axis(grid, (jnp.arange(top)[None, :] + rotation) % top, axis=1)


def load_shares(number_of, total, reach, lean, full):
    loads = [(1 << 20) // math.isqrt(grade ** lean) + 1 for grade in range(1, number_of + 1)]
    largest = reach if full else min(reach, max(-(-total // number_of), total * loads[0] // sum(loads)))
    least = 1 if total - largest >= number_of - 1 else 0
    given, spare = [largest] + [least] * (number_of - 1), total - largest - least * (number_of - 1)
    while spare > 0:
        free = [i for i in range(1, number_of) if given[i] < largest] or [i for i in range(1, number_of) if given[i] < reach]
        pool, left = sum([loads[i] for i in free]), spare
        for i in free:
            addition = min(reach - given[i], max(1, left * loads[i] // pool), spare)
            given[i] = given[i] + addition
            spare = spare - addition
    return np.array(given)


def normal_values(key, dims, deviation, bound, cuts=(), kind=jnp.bfloat16):
    drawn = deviation * jax.random.normal(key, dims, jnp.float32)
    if cuts:
        drawn = drawn * block_scale(key, dims, cuts, -0.22, 0.18)
    return jnp.clip(drawn, -bound, bound).astype(kind)


def gaussian_with(key, shape, deviation, reach, cuts, heavy, kind=jnp.bfloat16):
    drawn = deviation * jax.random.normal(key, shape, jnp.float32)
    if cuts:
        drawn = drawn * block_scale(key, shape, cuts, -0.22, 0.18)
    return jnp.clip(raised(drawn, jax.random.fold_in(key, 3), *heavy), -reach, reach).astype(kind)


def setup_inputs(seed: int = 0) -> dict:
    key_list = jax.random.split(jax.random.key(seed), 15)
    moe_input = normal_values(key_list[0], (SEQUENCE_TOKENS, D), 1.0, 6.0, ((0, 32),))
    out_grad = gaussian_with(key_list[1], (SEQUENCE_TOKENS, D), 1.0, 6.0, ((0, 32), (1, 16)), (0, 1, 32, 2.75))
    expert_ids_keys = jax.random.split(jax.random.fold_in(key_list[2], 1), SEQUENCE_TOKENS // TOK_DEV)
    expert_ids_turns = jax.random.permutation(jax.random.fold_in(key_list[2], 3), SEQUENCE_TOKENS // TOK_DEV)
    expert_ids = jax.vmap(lambda own, number: deal_out(jax.random.fold_in(key_list[2], 2), own, number, TOK_DEV, EXPERTS, 2, CAP, 1))(expert_ids_keys, expert_ids_turns).reshape((SEQUENCE_TOKENS, 2))
    expert_weights = jnp.clip(0.1 + 0.79999997 * jax.random.uniform(key_list[3], (SEQUENCE_TOKENS, 2), jnp.float32) ** block_scale(key_list[3], (SEQUENCE_TOKENS, 2), ((0, 32),), -0.2, 0.2), 0.1, 0.9)
    w_gate = normal_values(key_list[4], (EXPERTS, D, FF), D ** -0.5, 0.125, ((0, 32), (2, 16)))
    w_up = normal_values(key_list[5], (EXPERTS, D, FF), D ** -0.5, 0.125, ((0, 32), (2, 16)))
    w_down = normal_values(key_list[6], (EXPERTS, FF, D), FF ** -0.5, 0.125, ((0, 32), (1, 16)))
    out_proj = normal_values(key_list[7], (RET_WIDTH, D), RET_WIDTH ** -0.5, 0.15625, ((0, 16),))
    retained = normal_values(key_list[8], (SEQUENCE_TOKENS, RET_WIDTH), 1.0, 6.0, ((0, 32), (1, 16)))
    queries = normal_values(key_list[9], (SEQUENCE_TOKENS, KEY_WIDTH), 1.0, 6.0, ((0, 32), (1, 16)))
    keys = normal_values(key_list[10], (SEQUENCE_TOKENS, KEY_WIDTH), (KEY_DIM ** -0.5), 0.86328125, ((0, 32), (1, 16)))
    values = normal_values(key_list[11], (SEQUENCE_TOKENS, RET_WIDTH), 1.0, 6.0, ((0, 32), (1, 16)))
    log_decay = draw_log_decay(jax.random.fold_in(key_list[14], 71), 0)
    incoming_state = normal_values(key_list[13], (N_SP, RETENTION_HEADS, KEY_DIM, VALUE_DIM), 1.0, 6.0, ((0, 32), (1, 16)), jnp.float32)
    return dict(moe_input=moe_input, out_grad=out_grad, expert_ids=expert_ids, expert_weights=expert_weights, w_gate=w_gate, w_up=w_up, w_down=w_down, out_proj=out_proj, retained=retained, queries=queries, keys=keys, values=values, log_decay=log_decay, incoming_state=incoming_state)


def slot_table(expert_ids, expert_weights):
    per_block = expert_ids.reshape(N_SP, 2 * TOK_DEV)
    block_weights = expert_weights.reshape(N_SP, 2 * TOK_DEV)
    onehot = (per_block[:, :, None] == jnp.arange(EXPERTS, dtype=jnp.int32)[None, None, :]).astype(jnp.int32)
    ranks = jnp.sum((jnp.cumsum(onehot, axis=1) - onehot) * onehot, axis=2).astype(jnp.int32)
    block = jnp.arange(N_SP, dtype=jnp.int32)[:, None]
    dest = (per_block * (N_SP * CAP) + block * CAP + ranks).reshape(-1).astype(jnp.int32)
    token = (block * TOK_DEV + jnp.arange(2 * TOK_DEV, dtype=jnp.int32)[None, :] // 2).reshape(-1).astype(jnp.int32)
    table = jnp.full((EXPERTS * N_SP * CAP,), SEQUENCE_TOKENS, jnp.int32).at[dest].set(token)
    weight = jnp.zeros((EXPERTS * N_SP * CAP,), jnp.float32).at[dest].set(block_weights.reshape(-1))
    return table.reshape(EXPERTS, N_SP * CAP), weight.reshape(EXPERTS, N_SP * CAP)


def reference(moe_input, out_grad, expert_ids, expert_weights, w_gate, w_up, w_down, out_proj,
              retained, queries, keys, values, log_decay, incoming_state):
    f32 = jnp.float32
    bf16 = jnp.bfloat16
    upper_limit = lax.Precision.HIGHEST
    table, weight = slot_table(expert_ids, expert_weights)
    padded_rows = jnp.concatenate([moe_input, jnp.zeros((1, D), bf16)], axis=0)
    padded_grad = jnp.concatenate([out_grad, jnp.zeros((1, D), bf16)], axis=0)
    part = FF // N_TP

    def expert_back(args):
        index, slot_weight, gate_w, up_w, down_w = args
        rows = padded_rows[index]
        grad = (padded_grad[index].astype(f32) * slot_weight[:, None]).astype(bf16)
        gate = jnp.dot(rows, gate_w, preferred_element_type=f32)
        up = jnp.dot(rows, up_w, preferred_element_type=f32)
        sig = jax.nn.sigmoid(gate)
        swish = gate * sig
        act = (swish * up).astype(bf16)
        act_grad = jnp.dot(grad, down_w.T, preferred_element_type=f32)
        gate_grad = (act_grad * up * sig * (1.0 + gate * (1.0 - sig))).astype(bf16)
        up_grad = (act_grad * swish).astype(bf16)
        down_grad = jnp.dot(act.T, grad, preferred_element_type=f32).astype(bf16)
        gate_w_grad = jnp.dot(rows.T, gate_grad, preferred_element_type=f32).astype(bf16)
        up_w_grad = jnp.dot(rows.T, up_grad, preferred_element_type=f32).astype(bf16)
        slots = rows.shape[0]
        parts = (jnp.einsum('snf,dnf->nsd', gate_grad.astype(f32).reshape(slots, N_TP, part),
                            gate_w.astype(f32).reshape(D, N_TP, part))
                 + jnp.einsum('snf,dnf->nsd', up_grad.astype(f32).reshape(slots, N_TP, part),
                              up_w.astype(f32).reshape(D, N_TP, part)))
        rounded = lax.optimization_barrier(parts.astype(bf16))
        slot_in = jnp.sum(rounded.astype(f32), axis=0).astype(bf16)
        return gate_w_grad, up_w_grad, down_grad, slot_in

    w_gate_grad, w_up_grad, w_down_grad, slot_in = lax.map(expert_back, (table, weight, w_gate, w_up, w_down))
    token_grad = jnp.zeros((SEQUENCE_TOKENS + 1, D), f32).at[table.reshape(-1)].add(
        slot_in.reshape(-1, D).astype(f32))[:SEQUENCE_TOKENS]
    stream = (out_grad.astype(f32) + token_grad).astype(bf16)
    ret_grad = jnp.dot(stream, out_proj.T, preferred_element_type=f32).astype(bf16)
    out_proj_grad = jnp.dot(stream.T, retained, preferred_element_type=f32)

    q = queries.astype(f32).reshape(N_SP, TOK_DEV, RETENTION_HEADS, KEY_DIM)
    k = keys.astype(f32).reshape(N_SP, TOK_DEV, RETENTION_HEADS, KEY_DIM)
    v = values.astype(f32).reshape(N_SP, TOK_DEV, RETENTION_HEADS, VALUE_DIM)
    o = ret_grad.astype(f32).reshape(N_SP, TOK_DEV, RETENTION_HEADS, VALUE_DIM)
    b = jnp.cumsum(log_decay.reshape(N_SP, TOK_DEV, RETENTION_HEADS), axis=1)
    b_end = b[:, -1]
    diff = b[:, :, None, :] - b[:, None, :, :]
    place = jnp.arange(TOK_DEV)
    causal = (place[:, None] >= place[None, :])[None, :, :, None]
    decay = jnp.where(causal, jnp.exp(jnp.minimum(diff, 0.0)), 0.0)
    scores = jnp.einsum('nthk,nshk->ntsh', q, k, precision=upper_limit) * decay
    prob_grad = jnp.einsum('nthv,nshv->ntsh', o, v, precision=upper_limit) * decay
    added_input = jnp.einsum('nth,nthk,nthv->nhkv', jnp.exp(b), q, o, precision=upper_limit)

    def back_step(carry, inputs):
        factor, term = inputs
        return term + factor[:, None, None] * carry, carry

    _, state_gradient = lax.scan(back_step, jnp.zeros((RETENTION_HEADS, KEY_DIM, VALUE_DIM), f32),
                             (jnp.exp(b_end), added_input), reverse=True)
    tail = jnp.exp(b_end[:, None, :] - b)[..., None]
    query_grad = (jnp.einsum('ntsh,nshk->nthk', prob_grad, k, precision=upper_limit)
                  + jnp.exp(b)[..., None] * jnp.einsum('nthv,nhkv->nthk', o, incoming_state, precision=upper_limit))
    key_grad = (jnp.einsum('ntsh,nthk->nshk', prob_grad, q, precision=upper_limit)
                + tail * jnp.einsum('nshv,nhkv->nshk', v, state_gradient, precision=upper_limit))
    value_grad = (jnp.einsum('ntsh,nthv->nshv', scores, o, precision=upper_limit)
                  + tail * jnp.einsum('nshk,nhkv->nshv', k, state_gradient, precision=upper_limit))
    return (w_gate_grad, w_up_grad, w_down_grad, out_proj_grad,
            query_grad.reshape(SEQUENCE_TOKENS, KEY_WIDTH).astype(bf16),
            key_grad.reshape(SEQUENCE_TOKENS, KEY_WIDTH).astype(bf16),
            value_grad.reshape(SEQUENCE_TOKENS, RET_WIDTH).astype(bf16))
```

```python
import jax
import jax.numpy as jnp
from jax import lax
from jax.sharding import Mesh
from jax.sharding import PartitionSpec as P

TP = ("y", "c")
F32 = jnp.float32
BF16 = jnp.bfloat16
ACROSS = (((1,), (1,)), ((), ()))
ALONG = (((0,), (0,)), ((), ()))
SWAP = [(0, 1), (1, 0)]


def dot(a, b, dims=(((1,), (0,)), ((), ()))):
    return lax.dot_general(a, b, dims, preferred_element_type=F32)


def slot_tables(expert_ids, expert_weights, experts, capacity, padded):
    tokens = expert_ids.shape[0]
    ids = expert_ids.T
    weights = expert_weights.T
    names = jnp.arange(experts, dtype=jnp.int32)[:, None]
    onehot = [(names == ids[j][None, :]).astype(BF16) for j in (0, 1)]
    place = jnp.arange(tokens)
    earlier = (place[:, None] < place[None, :]).astype(BF16)
    before = dot(onehot[0] + onehot[1], earlier)
    slots = jnp.arange(experts * padded, dtype=jnp.int32)[:, None]
    picker, slot_weight = 0.0, 0.0
    for j in (0, 1):
        rank = jnp.sum(before * onehot[j].astype(F32), axis=0).astype(jnp.int32)
        hits = slots == (ids[j] * padded + rank)[None, :]
        picker = picker + jnp.where(hits, 1.0, 0.0)
        slot_weight = slot_weight + jnp.sum(
            jnp.where(hits, weights[j][None, :], 0.0), axis=1, keepdims=True
        )
    return picker.astype(BF16), slot_weight


def parity_columns(x, index):
    rows, cols = x.shape
    return lax.dynamic_index_in_dim(
        x.reshape(rows, 8, 2, cols // 16), index, 2, keepdims=False
    ).reshape(rows, cols // 2)


def parity_rows(x, index):
    rows, cols = x.shape
    return lax.dynamic_index_in_dim(
        x.reshape(8, 2, rows // 16, cols), index, 1, keepdims=False
    ).reshape(rows // 2, cols)


def joined_rows(own, other, core):
    rows, cols = own.shape
    own, other = (a.reshape(8, 1, rows // 8, cols) for a in (own, other))
    first = jnp.where(core == 0, own, other)
    second = jnp.where(core == 0, other, own)
    return jnp.concatenate([first, second], axis=1).reshape(2 * rows, cols)


def joined_columns(own, other, core):
    rows, cols = own.shape
    own, other = (a.reshape(rows, 8, 1, cols // 8) for a in (own, other))
    first = jnp.where(core == 0, own, other)
    second = jnp.where(core == 0, other, own)
    return jnp.concatenate([first, second], axis=2).reshape(rows, 2 * cols)


def in_three(x):
    high = x.astype(BF16)
    rest = x - high.astype(F32)
    middle = rest.astype(BF16)
    low = (rest - middle.astype(F32)).astype(BF16)
    return high, middle, low


def on_device(
    moe_input,
    out_grad,
    expert_ids,
    expert_weights,
    w_gate,
    w_up,
    w_down,
    out_proj,
    retained,
    queries,
    keys,
    values,
    log_decay,
    incoming_state,
):
    tokens = moe_input.shape[0]
    width = moe_input.shape[1]
    sp_count = lax.axis_size("sp")
    capacity = 5 * tokens // (2 * sp_count)
    padded = 16
    slot_count = sp_count * capacity
    core = lax.axis_index("c")
    block = lax.axis_index("sp")
    chunk = out_grad.shape[1]

    running = jnp.cumsum(log_decay[:, 0])
    last = running[-1]

    picker, slot_weight = slot_tables(expert_ids, expert_weights, sp_count, capacity, padded)
    mine = parity_columns(moe_input, core)
    send_rows = dot(picker, mine).astype(BF16).reshape(sp_count, padded, -1)
    parts = in_three(last)
    lane = jnp.arange(chunk)[None, None, :]
    extra = jnp.where(
        lane == 0, parts[0], jnp.where(lane == 1, parts[1], jnp.where(lane == 2, parts[2], 0.0))
    ).astype(BF16)
    send_grad = (dot(picker, out_grad) * slot_weight).astype(BF16).reshape(sp_count, padded, -1)
    spot = jnp.arange(padded)[None, :, None]
    send_grad = jnp.where(spot == padded - 1, extra, send_grad)

    got_grad = lax.all_to_all(send_grad, "sp", 0, 0, tiled=True)
    got_rows = lax.all_to_all(send_rows, "sp", 0, 0, tiled=True)
    rows_own = got_rows[:, :capacity].reshape(slot_count, -1)
    grad_part = got_grad[:, :capacity].reshape(slot_count, -1)
    ends = jnp.sum(got_grad[:, capacity, :3].astype(F32), axis=1)
    grad_own = lax.all_gather(grad_part, "y", axis=1, tiled=True)
    rows_other = lax.ppermute(rows_own, "c", SWAP)
    grad_other = lax.ppermute(grad_own, "c", SWAP)

    gate_own, gate_other = (parity_rows(w_gate[0], k) for k in (core, 1 - core))
    up_own, up_other = (parity_rows(w_up[0], k) for k in (core, 1 - core))
    down_own, down_other = (parity_columns(w_down[0], k) for k in (core, 1 - core))
    gate = dot(rows_own, gate_own) + dot(rows_other, gate_other)
    up = dot(rows_own, up_own) + dot(rows_other, up_other)
    sig = jax.nn.sigmoid(gate)
    swish = gate * sig
    act = (swish * up).astype(BF16)
    act_grad = dot(grad_own, down_own, ACROSS) + dot(grad_other, down_other, ACROSS)
    gate_grad = (act_grad * up * sig * (1.0 + gate * (1.0 - sig))).astype(BF16)
    up_grad = (act_grad * swish).astype(BF16)

    partial_other = (
        dot(gate_grad, gate_other, ACROSS) + dot(up_grad, up_other, ACROSS)
    ).astype(BF16)
    arrived = lax.ppermute(partial_other, "c", SWAP)
    partial_own = dot(gate_grad, gate_own, ACROSS) + dot(up_grad, up_own, ACROSS)
    pair = (partial_own + arrived.astype(F32)).astype(BF16)
    pieces = jnp.moveaxis(pair.reshape(slot_count, 8, chunk), 1, 0)
    pieces = lax.all_to_all(pieces, "y", 0, 0, tiled=True)
    share = jnp.sum(pieces.astype(F32), axis=0).astype(BF16)

    gate_w_grad = joined_rows(
        dot(rows_own, gate_grad, ALONG).astype(BF16),
        dot(rows_other, gate_grad, ALONG).astype(BF16),
        core,
    )
    up_w_grad = joined_rows(
        dot(rows_own, up_grad, ALONG).astype(BF16),
        dot(rows_other, up_grad, ALONG).astype(BF16),
        core,
    )
    down_grad = joined_columns(
        dot(act, grad_own, ALONG).astype(BF16), dot(act, grad_other, ALONG).astype(BF16), core
    )

    returned = lax.all_to_all(
        share.reshape(sp_count, capacity, chunk), "sp", 0, 0, tiled=True
    )
    returned = jnp.pad(returned, ((0, 0), (0, padded - capacity), (0, 0)))
    token_grad = dot(picker, returned.reshape(sp_count * padded, chunk), ALONG)
    stream_part = (out_grad.astype(F32) + token_grad).astype(BF16)
    stream = lax.all_gather(stream_part, TP, axis=1, tiled=True)
    ret_grad = dot(stream, out_proj, ACROSS).astype(BF16)

    q, k, v, o = (a.astype(F32) for a in (queries, keys, values, ret_grad))
    rising = jnp.exp(running)[:, None]
    inject = dot(q * rising, o, ALONG)
    value_dim = values.shape[1]
    sent = jnp.broadcast_to(inject.astype(BF16)[None], (sp_count, *inject.shape))
    states = lax.all_to_all(sent, "sp", 0, 0, tiled=True)
    proj_part = dot(stream, retained, ALONG).astype(BF16)
    proj_parts = lax.all_to_all(
        proj_part.reshape(sp_count, width // sp_count, value_dim), "sp", 0, 0, tiled=True
    )
    out_proj_grad = jnp.sum(proj_parts.astype(F32), axis=0)

    order = jnp.arange(sp_count)
    between = (order[None, :] > block) & (order[None, :] < order[:, None])
    factors = jnp.where(
        order > block, jnp.exp(jnp.sum(jnp.where(between, ends[None, :], 0.0), axis=1)), 0.0
    )
    state_grad = jnp.sum(factors[:, None, None] * states.astype(F32), axis=0)

    place = jnp.arange(tokens)
    causal = place[:, None] >= place[None, :]
    diff = running[:, None] - running[None, :]
    decay = jnp.where(causal, jnp.exp(jnp.minimum(diff, 0.0)), 0.0)
    scores = dot(q, k, ACROSS) * decay
    prob_grad = dot(o, v, ACROSS) * decay
    tail = jnp.exp(last - running)[:, None]
    query_grad = dot(prob_grad, k) + rising * dot(o, incoming_state[0, 0], ACROSS)
    key_grad = dot(prob_grad, q, ALONG) + tail * dot(v, state_grad, ACROSS)
    value_grad = dot(scores, o, ALONG) + tail * dot(k, state_grad)
    return (
        gate_w_grad[None],
        up_w_grad[None],
        down_grad[None],
        out_proj_grad,
        query_grad.astype(BF16),
        key_grad.astype(BF16),
        value_grad.astype(BF16),
    )


def solution(mesh):
    torus = Mesh(mesh.devices.reshape(mesh.shape["sp"], 8, 2), ("sp", "y", "c"))
    placed = (
        P("sp", None),
        P("sp", TP),
        P("sp", None),
        P("sp", None),
        P("sp", None, TP),
        P("sp", None, TP),
        P("sp", TP, None),
        P(TP, None),
        P("sp", TP),
        P("sp", TP),
        P("sp", TP),
        P("sp", TP),
        P("sp", TP),
        P("sp", TP, None, None),
    )
    return jax.shard_map(
        on_device,
        mesh=torus,
        in_specs=placed,
        out_specs=(
            P("sp", None, TP),
            P("sp", None, TP),
            P("sp", TP, None),
            P("sp", TP),
            P("sp", TP),
            P("sp", TP),
            P("sp", TP),
        ),
        check_vma=False,
    )
```

```python
import functools

import jax
import jax.numpy as jnp
from jax import lax
from jax.experimental import pallas as pl
from jax.experimental.pallas import tpu as pltpu
from jax.sharding import Mesh
from jax.sharding import PartitionSpec as P

TP = ("y", "c")
F32 = jnp.float32
BF16 = jnp.bfloat16
PLAIN = (((1,), (0,)), ((), ()))
ACROSS = (((1,), (1,)), ((), ()))
ALONG = (((0,), (0,)), ((), ()))
SWAP = [(0, 1), (1, 0)]
VMEM = pl.BlockSpec(memory_space=pltpu.VMEM)
SMEM = pl.BlockSpec(memory_space=pltpu.SMEM)


def dot(a, b, dims=PLAIN):
    return lax.dot_general(a, b, dims, preferred_element_type=F32)


def call(body, ins, outs, name, scratch=(), flops=0, limit=20):
    specs = [SMEM if k == "s" else VMEM for k, _ in ins]
    arrays = [a for _, a in ins]
    return pl.pallas_call(
        body,
        in_specs=specs,
        out_specs=tuple(VMEM for _ in outs),
        out_shape=tuple(jax.ShapeDtypeStruct(s, d) for s, d in outs),
        scratch_shapes=list(scratch),
        name=name,
        compiler_params=pltpu.CompilerParams(vmem_limit_bytes=limit << 20),
        cost_estimate=pl.CostEstimate(flops=flops, transcendentals=0, bytes_accessed=0),
    )(*arrays)


def in_three(x):
    high = x.astype(BF16)
    rest = x - high.astype(F32)
    middle = rest.astype(BF16)
    low = (rest - middle.astype(F32)).astype(BF16)
    return high, middle, low


def setup_body(ids_ref, weight_ref, grad_ref, picker_ref, send_ref, *, experts, padded):
    tokens = ids_ref.shape[1]
    slots = experts * padded
    grad = grad_ref[...].astype(F32)
    row = lax.broadcasted_iota(jnp.int32, (tokens, tokens), 0)
    col = lax.broadcasted_iota(jnp.int32, (tokens, tokens), 1)
    same = jnp.where(row == col, 1.0, 0.0).astype(BF16)
    earlier = jnp.where(row > col, 1.0, 0.0).astype(BF16)
    lines = jnp.concatenate(
        [ids_ref[...].astype(F32)] + [p.astype(F32) for p in in_three(weight_ref[...])], axis=0
    )
    columns = dot(same, lines.astype(BF16), ACROSS)
    ids = columns[:, :2]
    names = lax.broadcasted_iota(jnp.int32, (tokens, experts), 1).astype(F32)
    onehot = [jnp.where(ids[:, j : j + 1] == names, 1.0, 0.0) for j in (0, 1)]
    before = dot(earlier, (onehot[0] + onehot[1]).astype(BF16))
    spots = lax.broadcasted_iota(jnp.int32, (tokens, slots), 1)
    picker, sent = None, None
    for j in (0, 1):
        rank = jnp.sum(before * onehot[j], axis=1, keepdims=True)
        slot = (ids[:, j : j + 1] * padded + rank).astype(jnp.int32)
        hits = jnp.where(spots == slot, 1.0, 0.0).astype(BF16)
        high, middle, low = (columns[:, k + j : k + j + 1] for k in (2, 4, 6))
        weight = (high + middle) + low
        part = dot(hits, (grad * weight).astype(BF16), ALONG)
        picker = hits if picker is None else picker + hits
        sent = part if sent is None else sent + part
    picker_ref[...] = picker
    send_ref[...] = sent.astype(BF16)


def rows_body(core_ref, picker_ref, input_ref, decay_ref, send_ref, *, padded):
    rows = dot(picker_ref[...], half_columns(input_ref, core_ref[0]), ALONG)
    parts = in_three(jnp.sum(decay_ref[...], axis=1, keepdims=True))
    lane = lax.broadcasted_iota(jnp.int32, rows.shape, 1)
    row = lax.broadcasted_iota(jnp.int32, rows.shape, 0)
    extra = jnp.zeros((1, 1), F32)
    for k, part in enumerate(parts):
        extra = jnp.where(lane == k, part.astype(F32), extra)
    send_ref[...] = jnp.where((row & (padded - 1)) == padded - 1, extra, rows).astype(BF16)


def half_weights(ref, core):
    chunks = ref[:, core]
    return chunks.reshape(chunks.shape[0] * chunks.shape[1], chunks.shape[2])


def half_columns(ref, core):
    chunk = 128
    pieces = [
        ref[:, pl.ds(pl.multiple_of((2 * k + core) * chunk, chunk), chunk)]
        for k in range(ref.shape[1] // (2 * chunk))
    ]
    return jnp.concatenate(pieces, axis=1)


def own_body(core_ref, rows_ref, grad_ref, gate_ref, up_ref, down_ref, hidden_ref, back_ref):
    core = core_ref[0]
    both = jnp.concatenate([half_weights(gate_ref, core), half_weights(up_ref, core)], axis=1)
    hidden_ref[...] = dot(rows_ref[...], both)
    back_ref[...] = dot(grad_ref[...], half_columns(down_ref, core), ACROSS)


def other_body(
    core_ref, rows_ref, grad_ref, gate_ref, up_ref, down_ref, hidden_ref, back_ref,
    act_ref, both_ref, full_ref,
):
    core = 1 - core_ref[0]
    short = grad_ref.shape[0]
    both = jnp.concatenate([half_weights(gate_ref, core), half_weights(up_ref, core)], axis=1)
    hidden = hidden_ref[...] + dot(rows_ref[...], both)
    full_ref[pl.ds(full_ref.shape[0] - 8, 8), :] = jnp.zeros((8, full_ref.shape[1]), F32)
    full_ref[pl.ds(0, short), :] = back_ref[...] + dot(
        grad_ref[...], half_columns(down_ref, core), ACROSS
    )
    act_grad = full_ref[...]
    units = act_grad.shape[1]
    gate, up = hidden[:, :units], hidden[:, units:]
    sig = jax.nn.sigmoid(gate)
    swish = gate * sig
    act_ref[...] = (swish * up).astype(BF16)[:short]
    both_ref[:, :units] = (act_grad * up * sig * (1.0 + gate * (1.0 - sig))).astype(BF16)
    both_ref[:, units:] = (act_grad * swish).astype(BF16)


def input_grad_body(core_ref, mine_ref, pair_ref, gate_ref, up_ref, cross_ref, out_ref):
    core = core_ref[0]
    grads = jnp.concatenate([mine_ref[...], pair_ref[...]], axis=1)
    gate, up, cross = gate_ref[:, core], up_ref[:, core], cross_ref[...]
    weights = jnp.concatenate([gate, up, cross], axis=2)
    for k in range(0, weights.shape[0], 2):
        two = weights[k : k + 2].reshape(2 * weights.shape[1], weights.shape[2])
        found = dot(grads, two, ACROSS).astype(BF16)
        out_ref[k] = found[:, : weights.shape[1]]
        out_ref[k + 1] = found[:, weights.shape[1] :]


def sum_body(parts_ref, out_ref):
    total = parts_ref[0].astype(F32)
    for k in range(1, parts_ref.shape[0]):
        total = total + parts_ref[k].astype(F32)
    out_ref[...] = total.astype(BF16)


def pack_body(stream_ref, proj_ref, kept_ref, query_ref, rising_ref, ret_ref, pay_ref):
    stream = stream_ref[...]
    ret = dot(stream, proj_ref[...], ACROSS).astype(BF16)
    ret_ref[...] = ret
    inject = dot((query_ref[...].astype(F32) * rising_ref[...]).astype(BF16), ret, ALONG)
    proj = dot(stream, kept_ref[...], ALONG)
    count, rows, lanes = pay_ref.shape
    each = proj.shape[0] // count
    width = proj.shape[1]
    whole = rows - inject.shape[0]
    rest = each - whole
    fold = lanes - width
    blank = jnp.zeros((rows - rest * (width // fold), fold), F32)
    for m in range(count):
        own = proj[m * each : (m + 1) * each]
        left = jnp.concatenate([inject, own[:whole]], axis=0)
        right = jnp.concatenate(
            [own[whole:, k * fold : (k + 1) * fold] for k in range(width // fold)] + [blank],
            axis=0,
        )
        pay_ref[m] = jnp.concatenate([left, right], axis=1).astype(BF16)


def last_body(
    factor_ref, got_ref, keys_ref, values_ref, tail_ref, tail_row_ref, key_part_ref,
    value_part_ref, key_ref, value_ref, proj_ref,
):
    count, rows, lanes = got_ref.shape
    key_dim, width = keys_ref.shape[1], values_ref.shape[1]
    state, total = None, None
    for m in range(count):
        part = got_ref[m].astype(F32)
        total = part if total is None else total + part
        scaled = factor_ref[m] * part[:key_dim]
        state = scaled if state is None else state + scaled
    state = state[:, :width].astype(BF16)
    fold = lanes - width
    whole = rows - key_dim
    rest = proj_ref.shape[0] - whole
    proj_ref[:whole, :] = total[key_dim:, :width]
    proj_ref[whole:, :] = jnp.concatenate(
        [total[k * rest : (k + 1) * rest, width:] for k in range(width // fold)], axis=1
    )
    tail = tail_ref[...]
    across = dot(state, values_ref[...], ACROSS)
    key_ref[...] = (key_part_ref[...] + tail_row_ref[...] * across).astype(BF16)
    value_ref[...] = (value_part_ref[...] + tail * dot(keys_ref[...], state)).astype(BF16)


def parity_columns(x, index):
    rows, cols = x.shape
    return lax.dynamic_index_in_dim(
        x.reshape(rows, 8, 2, cols // 16), index, 2, keepdims=False
    ).reshape(rows, cols // 2)


def joined_rows(own, other, core):
    rows, cols = own.shape
    own, other = (a.reshape(8, 1, rows // 8, cols) for a in (own, other))
    first = jnp.where(core == 0, own, other)
    second = jnp.where(core == 0, other, own)
    return jnp.concatenate([first, second], axis=1).reshape(2 * rows, cols)


def joined_columns(own, other, core):
    rows, cols = own.shape
    own, other = (a.reshape(rows, 8, 1, cols // 8) for a in (own, other))
    first = jnp.where(core == 0, own, other)
    second = jnp.where(core == 0, other, own)
    return jnp.concatenate([first, second], axis=2).reshape(rows, 2 * cols)


def on_device(
    moe_input,
    out_grad,
    expert_ids,
    expert_weights,
    w_gate,
    w_up,
    w_down,
    out_proj,
    retained,
    queries,
    keys,
    values,
    log_decay,
    incoming_state,
):
    tokens, width = moe_input.shape
    sp_count = lax.axis_size("sp")
    padded = 16
    slots = sp_count * padded
    short = slots - 1
    core = lax.axis_index("c")
    block = lax.axis_index("sp")
    chunk = out_grad.shape[1]
    half = width // 2
    units = w_gate.shape[2]
    key_dim, value_dim = queries.shape[1], values.shape[1]

    core_1 = core.astype(jnp.int32).reshape(1)
    picker, send_grad = call(
        functools.partial(setup_body, experts=sp_count, padded=padded),
        [("v", expert_ids.T), ("v", expert_weights.T), ("v", out_grad)],
        [((tokens, slots), BF16), ((slots, chunk), BF16)],
        "setup",
    )
    with jax.named_scope("grad_send"):
        got_grad = lax.all_to_all(
            send_grad.reshape(sp_count, padded, chunk), "sp", 0, 0, tiled=True
        )
    got_grad = got_grad.reshape(slots, chunk)[:short]

    (send_rows,) = call(
        functools.partial(rows_body, padded=padded),
        [("s", core_1), ("v", picker), ("v", moe_input), ("v", log_decay.T)],
        [((slots, half), BF16)],
        "rows",
    )
    gate_4 = w_gate.reshape(8, 2, chunk, units)
    up_4 = w_up.reshape(8, 2, chunk, units)
    down_2 = w_down[0]
    cross_sent = jnp.concatenate(
        [lax.dynamic_index_in_dim(w, 1 - core, 1, keepdims=False) for w in (gate_4, up_4)], axis=2
    )
    with jax.named_scope("cross_send"):
        cross = lax.ppermute(cross_sent, "c", SWAP)

    send_rows, got_grad, cross = lax.optimization_barrier((send_rows, got_grad, cross))
    send_rows = send_rows.reshape(sp_count, padded, half)
    with jax.named_scope("rows_send"):
        got_rows = lax.all_to_all(send_rows, "sp", 0, 0, tiled=True)
    ends = jnp.sum(got_rows[:, padded - 1, :3].astype(F32), axis=1)
    rows_own = got_rows.reshape(slots, half)
    running = jnp.cumsum(log_decay[:, 0])
    last = running[-1]

    with jax.named_scope("grad_gather"):
        grad_own = lax.all_gather(got_grad, "y", axis=1, tiled=True)
    rows_own, grad_own = lax.optimization_barrier((rows_own, grad_own))
    rows_other = lax.ppermute(rows_own, "c", SWAP)
    grad_other = lax.ppermute(grad_own, "c", SWAP)

    hidden, back = call(
        own_body,
        [("s", core_1), ("v", rows_own), ("v", grad_own), ("v", gate_4), ("v", up_4), ("v", down_2)],
        [((slots, 2 * units), F32), ((short, units), F32)],
        "own_half",
        flops=6 * slots * half * units,
    )
    act, both = call(
        other_body,
        [
            ("s", core_1), ("v", rows_other), ("v", grad_other), ("v", gate_4), ("v", up_4),
            ("v", down_2), ("v", hidden), ("v", back),
        ],
        [((short, units), BF16), ((slots, 2 * units), BF16)],
        "other_half",
        scratch=[pltpu.VMEM((slots, units), F32)],
        flops=6 * slots * half * units,
    )
    pair_both = lax.ppermute(both, "c", SWAP)
    (pieces,) = call(
        input_grad_body,
        [
            ("s", core_1), ("v", both), ("v", pair_both), ("v", gate_4), ("v", up_4), ("v", cross),
        ],
        [((8, slots, chunk), BF16)],
        "input_grad",
        flops=8 * slots * half * units,
    )
    pieces = lax.all_to_all(pieces, "y", 0, 0, tiled=True)

    w_own, w_other = (dot(r, both, ALONG).astype(BF16) for r in (rows_own, rows_other))
    w_grads = joined_rows(w_own, w_other, core)
    gate_w_grad, up_w_grad = w_grads[:, :units], w_grads[:, units:]
    down_grad = joined_columns(
        dot(act, grad_own, ALONG).astype(BF16), dot(act, grad_other, ALONG).astype(BF16), core
    )

    (share,) = call(sum_body, [("v", pieces)], [((slots, chunk), BF16)], "add_parts")
    returned = lax.all_to_all(
        share.reshape(sp_count, padded, chunk), "sp", 0, 0, tiled=True
    ).reshape(slots, chunk)
    stream_part = (out_grad.astype(F32) + dot(picker, returned)).astype(BF16)
    stream = lax.all_gather(stream_part, TP, axis=1, tiled=True)

    rising = jnp.exp(running)[:, None]
    whole = 40
    ret_grad, payload = call(
        pack_body,
        [("v", stream), ("v", out_proj), ("v", retained), ("v", queries), ("v", rising)],
        [((tokens, value_dim), BF16), ((sp_count, key_dim + whole, 128), BF16)],
        "pack",
        flops=4 * tokens * width * value_dim,
    )
    got = lax.all_to_all(payload, "sp", 0, 0, tiled=True)

    order = jnp.arange(sp_count)
    between = (order[None, :] > block) & (order[None, :] < order[:, None])
    factors = jnp.where(
        order > block, jnp.exp(jnp.sum(jnp.where(between, ends[None, :], 0.0), axis=1)), 0.0
    )
    q, k, v, o = (a.astype(F32) for a in (queries, keys, values, ret_grad))
    place = jnp.arange(tokens)
    causal = place[:, None] >= place[None, :]
    diff = running[:, None] - running[None, :]
    decay = jnp.where(causal, jnp.exp(jnp.minimum(diff, 0.0)), 0.0)
    scores = dot(q, k, ACROSS) * decay
    prob_grad = dot(o, v, ACROSS) * decay
    tail = jnp.exp(last - running)[:, None]
    query_grad = dot(prob_grad, k) + rising * dot(o, incoming_state[0, 0], ACROSS)
    key_part = dot(q, prob_grad, ALONG)
    value_part = dot(scores, o, ALONG)
    key_grad, value_grad, out_proj_grad = call(
        last_body,
        [
            ("s", factors), ("v", got), ("v", keys), ("v", values), ("v", tail),
            ("v", tail.T), ("v", key_part), ("v", value_part),
        ],
        [
            ((key_dim, tokens), BF16), ((tokens, value_dim), BF16),
            ((width // sp_count, value_dim), F32),
        ],
        "finish",
    )
    return (
        gate_w_grad[None],
        up_w_grad[None],
        down_grad[None],
        out_proj_grad,
        query_grad.astype(BF16),
        key_grad.T,
        value_grad,
    )


def solution(mesh):
    torus = Mesh(mesh.devices.reshape(mesh.shape["sp"], 8, 2), ("sp", "y", "c"))
    placed = (
        P("sp", None),
        P("sp", TP),
        P("sp", None),
        P("sp", None),
        P("sp", None, TP),
        P("sp", None, TP),
        P("sp", TP, None),
        P(TP, None),
        P("sp", TP),
        P("sp", TP),
        P("sp", TP),
        P("sp", TP),
        P("sp", TP),
        P("sp", TP, None, None),
    )
    return jax.shard_map(
        on_device,
        mesh=torus,
        in_specs=placed,
        out_specs=(
            P("sp", None, TP),
            P("sp", None, TP),
            P("sp", TP, None),
            P("sp", TP),
            P("sp", TP),
            P("sp", TP),
            P("sp", TP),
        ),
        check_vma=False,
    )
```

```python
import functools

import jax
import jax.numpy as jnp
from jax import lax
from jax.experimental import pallas as pl
from jax.experimental.pallas import tpu as pltpu
from jax.sharding import Mesh
from jax.sharding import PartitionSpec as P

TP = ("y", "c")
F32 = jnp.float32
BF16 = jnp.bfloat16
PLAIN = (((1,), (0,)), ((), ()))
ACROSS = (((1,), (1,)), ((), ()))
ALONG = (((0,), (0,)), ((), ()))
SWAP = [(0, 1), (1, 0)]
SWAP_TYPE = BF16
VMEM = pl.BlockSpec(memory_space=pltpu.VMEM)
SMEM = pl.BlockSpec(memory_space=pltpu.SMEM)
HBM = pl.BlockSpec(memory_space=pltpu.HBM)
PLACES = {"s": SMEM, "v": VMEM, "h": HBM}


def dot(a, b, dims=PLAIN):
    return lax.dot_general(a, b, dims, preferred_element_type=F32)


def call(body, ins, outs, scratch=(), flops=0, limit=20):
    specs = [PLACES[k] for k, _ in ins]
    places = tuple(PLACES[out[2] if len(out) > 2 else "v"] for out in outs)
    arrays = [
        pltpu.with_memory_space_constraint(a, pltpu.HBM) if k == "h" else a for k, a in ins
    ]
    return pl.pallas_call(
        body,
        in_specs=specs,
        out_specs=places,
        out_shape=tuple(
            pltpu.HBM(out[0], out[1]) if len(out) > 2 else jax.ShapeDtypeStruct(out[0], out[1])
            for out in outs
        ),
        scratch_shapes=list(scratch),
        compiler_params=pltpu.CompilerParams(vmem_limit_bytes=limit << 20),
        cost_estimate=pl.CostEstimate(flops=flops, transcendentals=0, bytes_accessed=0),
    )(*arrays)


def in_three(x):
    high = x.astype(BF16)
    rest = x - high.astype(F32)
    middle = rest.astype(BF16)
    low = (rest - middle.astype(F32)).astype(BF16)
    return high, middle, low


def started(pairs, sems):
    copies = [
        pltpu.make_async_copy(source, target, sems.at[k])
        for k, (source, target) in enumerate(pairs)
    ]
    for copy in copies:
        copy.start()
    return copies


def waited(copies):
    for copy in copies:
        copy.wait()


def setup_body(
    ids_hbm, weight_hbm, grad_hbm, picker_ref, send_ref, ids_ref, weight_ref, grad_ref, sems,
    *, experts, padded,
):
    waited(
        started([(ids_hbm, ids_ref), (weight_hbm, weight_ref), (grad_hbm, grad_ref)], sems)
    )
    tokens = ids_ref.shape[1]
    slots = experts * padded
    grad = grad_ref[...].astype(F32)
    row = lax.broadcasted_iota(jnp.int32, (tokens, tokens), 0)
    col = lax.broadcasted_iota(jnp.int32, (tokens, tokens), 1)
    same = jnp.where(row == col, 1.0, 0.0).astype(BF16)
    earlier = jnp.where(row > col, 1.0, 0.0).astype(BF16)
    lines = jnp.concatenate(
        [ids_ref[...].astype(F32)] + [p.astype(F32) for p in in_three(weight_ref[...])], axis=0
    )
    columns = dot(same, lines.astype(BF16), ACROSS)
    ids = columns[:, :2]
    names = lax.broadcasted_iota(jnp.int32, (tokens, experts), 1).astype(F32)
    onehot = [jnp.where(ids[:, j : j + 1] == names, 1.0, 0.0) for j in (0, 1)]
    before = dot(earlier, (onehot[0] + onehot[1]).astype(BF16))
    spots = lax.broadcasted_iota(jnp.int32, (tokens, slots), 1)
    picker, sent = None, None
    for j in (0, 1):
        rank = jnp.sum(before * onehot[j], axis=1, keepdims=True)
        slot = (ids[:, j : j + 1] * padded + rank).astype(jnp.int32)
        hits = jnp.where(spots == slot, 1.0, 0.0).astype(BF16)
        high, middle, low = (columns[:, k + j : k + j + 1] for k in (2, 4, 6))
        weight = (high + middle) + low
        part = dot(hits, (grad * weight).astype(BF16), ALONG)
        picker = hits if picker is None else picker + hits
        sent = part if sent is None else sent + part
    picker_ref[...] = picker
    send_ref[...] = sent.astype(BF16)


def rows_body(
    core_ref, picker_ref, input_hbm, decay_hbm, send_ref, input_ref, decay_ref, sems, *, padded
):
    waited(started([(input_hbm, input_ref), (decay_hbm, decay_ref)], sems))
    rows = dot(picker_ref[...], half_columns(input_ref, core_ref[0]), ALONG)
    parts = in_three(jnp.sum(decay_ref[...], axis=1, keepdims=True))
    lane = lax.broadcasted_iota(jnp.int32, rows.shape, 1)
    row = lax.broadcasted_iota(jnp.int32, rows.shape, 0)
    extra = jnp.zeros((1, 1), F32)
    for k, part in enumerate(parts):
        extra = jnp.where(lane == k, part.astype(F32), extra)
    send_ref[...] = jnp.where((row & (padded - 1)) == padded - 1, extra, rows).astype(BF16)


def half_columns(ref, core):
    chunk = 128
    pieces = [
        ref[:, pl.ds(pl.multiple_of((2 * k + core) * chunk, chunk), chunk)]
        for k in range(ref.shape[1] // (2 * chunk))
    ]
    return jnp.concatenate(pieces, axis=1)


def prep_body(
    core_ref, gate_hbm, up_hbm, down_hbm, mine_hbm, theirs_hbm, mine_ref, theirs_ref, sems, out_sems
):
    core = core_ref[0]
    count, chunk = gate_hbm.shape[0], gate_hbm.shape[2]
    pairs = []
    for target, half in ((theirs_ref, 1 - core), (mine_ref, core)):
        pairs += [(gate_hbm.at[:, half], target.at[0]), (up_hbm.at[:, half], target.at[1])]
        for k in range(count):
            at = pl.multiple_of((2 * k + half) * chunk, chunk)
            pairs.append((down_hbm.at[:, pl.ds(at, chunk)], target.at[2, k]))
    waited(started(pairs, sems))
    waited(started([(theirs_ref, theirs_hbm), (mine_ref, mine_hbm)], out_sems))


def side_by_side(refs):
    parts = [ref[k] for ref in refs for k in (0, 1)]
    return jnp.concatenate([p.reshape(-1, p.shape[2]) for p in parts], axis=1)


def lined_up(ref):
    return jnp.concatenate([ref[2, k] for k in range(ref.shape[1])], axis=1)


def own_body(rows_ref, grad_ref, mine_hbm, cross_ref, out_ref, mine_ref, sems):
    units = mine_ref.shape[3]
    short = grad_ref.shape[0]
    copies = started(
        [(mine_hbm.at[part], mine_ref.at[part]) for part in (pl.ds(2, 1), pl.ds(0, 2))], sems
    )
    waited(copies[:1])
    downs = jnp.concatenate([lined_up(mine_ref), lined_up(cross_ref)], axis=0)
    back = dot(grad_ref[...], downs, ACROSS).astype(out_ref.dtype)
    blank = jnp.zeros((8, units), out_ref.dtype)
    for k in (0, 1):
        at = 3 * units * k + 2 * units
        out_ref[pl.ds(out_ref.shape[0] - 8, 8), at : at + units] = blank
        out_ref[pl.ds(0, short), at : at + units] = back[:, units * k : units * (k + 1)]
    waited(copies[1:])
    hidden = dot(rows_ref[...], side_by_side((mine_ref, cross_ref))).astype(out_ref.dtype)
    for k in (0, 1):
        at = 3 * units * k
        out_ref[:, at : at + 2 * units] = hidden[:, 2 * units * k : 2 * units * (k + 1)]


def units_body(
    part_ref, pair_ref, mine_hbm, cross_ref, act_hbm, both_hbm, out_hbm,
    mine_ref, act_ref, both_ref, out_ref, sems, out_sems,
):
    units = mine_ref.shape[3]
    chunk = mine_ref.shape[2]
    short = act_ref.shape[0]
    copies = started([(mine_hbm.at[pl.ds(0, 2)], mine_ref)], sems)
    for k in (0, 1):
        at, there = 3 * units * k, 3 * units * (1 - k)
        gate, up, act_grad = (
            part_ref[:, at + j * units : at + (j + 1) * units].astype(F32)
            + pair_ref[:, there + j * units : there + (j + 1) * units].astype(F32)
            for j in range(3)
        )
        sig = jax.nn.sigmoid(gate)
        swish = gate * sig
        act_ref[:, k * units : (k + 1) * units] = (swish * up).astype(BF16)[:short]
        both_ref[:, 2 * k * units : (2 * k + 1) * units] = (
            act_grad * up * sig * (1.0 + gate * (1.0 - sig))
        ).astype(BF16)
        both_ref[:, (2 * k + 1) * units : (2 * k + 2) * units] = (act_grad * swish).astype(BF16)
    count = out_ref.shape[0]
    sent = []
    for k, (source, target) in enumerate([(act_ref, act_hbm), (both_ref, both_hbm)]):
        copy = pltpu.make_async_copy(source, target, out_sems.at[count + k])
        copy.start()
        sent.append(copy)
    waited(copies)
    grads = both_ref[...]
    for k in range(0, count, 2):
        two = jnp.concatenate(
            [
                ref[j, pl.ds(k, 2)].reshape(2 * chunk, units)
                for ref in (mine_ref, cross_ref)
                for j in (0, 1)
            ],
            axis=1,
        )
        part = dot(grads, two, ACROSS).astype(BF16)
        for j in (0, 1):
            out_ref[k + j] = part[:, chunk * j : chunk * (j + 1)]
            copy = pltpu.make_async_copy(out_ref.at[k + j], out_hbm.at[k + j], out_sems.at[k + j])
            copy.start()
            sent.append(copy)
    waited(sent)


def sum_body(parts_ref, out_ref):
    total = parts_ref[0].astype(F32)
    for k in range(1, parts_ref.shape[0]):
        total = total + parts_ref[k].astype(F32)
    out_ref[...] = total.astype(BF16)


def pack_body(stream_ref, proj_ref, kept_ref, query_ref, rising_ref, ret_ref, pay_ref):
    stream = stream_ref[...]
    ret = dot(stream, proj_ref[...], ACROSS).astype(BF16)
    ret_ref[...] = ret
    inject = dot(query_ref[...] * rising_ref[...], ret)
    proj = dot(kept_ref[...], stream, ALONG)
    lanes = pay_ref.shape[2]
    width = proj.shape[0]
    fold = lanes - width
    rows = pay_ref.shape[1] - width // 2
    rest = inject.shape[0] - rows
    side = [inject[rows:, k * fold : (k + 1) * fold] for k in range(width // fold)]
    blank = jnp.zeros((rows - rest * len(side), fold), F32)
    top = jnp.concatenate(
        [inject[:rows], jnp.concatenate(side + [blank], axis=0)], axis=1
    ).astype(BF16)
    low = lax.broadcasted_iota(jnp.int32, (width // 2, lanes), 1) < lanes // 2
    for j in range(proj.shape[1] // lanes):
        tile = proj[:, j * lanes : (j + 1) * lanes]
        upper, under = tile[: width // 2], tile[width // 2 :]
        turned = [pltpu.roll(t, lanes // 2, 1) for t in (upper, under)]
        pay_ref[2 * j, :rows] = top
        pay_ref[2 * j, rows:] = jnp.where(low, upper, turned[1]).astype(BF16)
        pay_ref[2 * j + 1, :rows] = top
        pay_ref[2 * j + 1, rows:] = jnp.where(low, turned[0], under).astype(BF16)


def last_body(
    factor_ref, got_ref, keys_ref, values_ref, tail_ref, tail_row_ref, key_part_ref,
    value_part_ref, key_ref, value_ref, proj_ref,
):
    count, _, lanes = got_ref.shape
    key_dim, width = keys_ref.shape[1], values_ref.shape[1]
    rows = got_ref.shape[1] - width // 2
    fold = lanes - width
    rest = key_dim - rows
    state, total = None, None
    for m in range(count):
        part = got_ref[m, rows:].astype(F32)
        total = part if total is None else total + part
        scaled = factor_ref[m] * got_ref[m, :rows].astype(F32)
        state = scaled if state is None else state + scaled
    state = jnp.concatenate(
        [
            state[:, :width],
            jnp.concatenate(
                [state[k * rest : (k + 1) * rest, width:] for k in range(width // fold)], axis=1
            ),
        ],
        axis=0,
    ).astype(BF16)
    half = lanes // 2
    proj_ref[...] = jnp.concatenate([total[:, :half], total[:, half:]], axis=0).T
    tail = tail_ref[...]
    across = dot(state, values_ref[...], ACROSS)
    key_ref[...] = (key_part_ref[...] + tail_row_ref[...] * across).astype(BF16)
    value_ref[...] = (value_part_ref[...] + tail * dot(keys_ref[...], state)).astype(BF16)


def joined_rows(own, other, core):
    rows, cols = own.shape
    own, other = (a.reshape(8, 1, rows // 8, cols) for a in (own, other))
    first = jnp.where(core == 0, own, other)
    second = jnp.where(core == 0, other, own)
    return jnp.concatenate([first, second], axis=1).reshape(2 * rows, cols)


def joined_columns(own, other, core):
    rows, cols = own.shape
    own, other = (a.reshape(rows, 8, 1, cols // 8) for a in (own, other))
    first = jnp.where(core == 0, own, other)
    second = jnp.where(core == 0, other, own)
    return jnp.concatenate([first, second], axis=2).reshape(rows, 2 * cols)


def on_device(
    moe_input,
    out_grad,
    expert_ids,
    expert_weights,
    w_gate,
    w_up,
    w_down,
    out_proj,
    retained,
    queries,
    keys,
    values,
    log_decay,
    incoming_state,
):
    tokens, width = moe_input.shape
    sp_count = lax.axis_size("sp")
    padded = 16
    slots = sp_count * padded
    short = slots - 1
    core = lax.axis_index("c")
    block = lax.axis_index("sp")
    chunk = out_grad.shape[1]
    half = width // 2
    units = w_gate.shape[2]
    key_dim, value_dim = queries.shape[1], values.shape[1]

    core_1 = core.astype(jnp.int32).reshape(1)
    picker, send_grad = call(
        functools.partial(setup_body, experts=sp_count, padded=padded),
        [("h", expert_ids.T), ("h", expert_weights.T), ("h", out_grad)],
        [((tokens, slots), BF16), ((slots, chunk), BF16)],
        scratch=[
            pltpu.VMEM((2, tokens), jnp.int32), pltpu.VMEM((2, tokens), F32),
            pltpu.VMEM((tokens, chunk), BF16), pltpu.SemaphoreType.DMA((3,)),
        ],
    )
    gate_4 = w_gate.reshape(8, 2, chunk, units)
    up_4 = w_up.reshape(8, 2, chunk, units)
    down_2 = w_down[0]
    halves = [((3, 8, chunk, units), BF16, "h")] * 2
    mine, theirs = call(
        prep_body,
        [("s", core_1), ("h", gate_4), ("h", up_4), ("h", down_2)],
        halves,
        scratch=[
            pltpu.VMEM((3, 8, chunk, units), BF16), pltpu.VMEM((3, 8, chunk, units), BF16),
            pltpu.SemaphoreType.DMA((20,)), pltpu.SemaphoreType.DMA((2,)),
        ],
    )
    cross = lax.ppermute(theirs, "c", SWAP)
    got_grad = lax.all_to_all(send_grad.reshape(sp_count, padded, chunk), "sp", 0, 0, tiled=True)
    got_grad = got_grad.reshape(slots, chunk)[:short]

    (send_rows,) = call(
        functools.partial(rows_body, padded=padded),
        [("s", core_1), ("v", picker), ("h", moe_input), ("h", log_decay.T)],
        [((slots, half), BF16)],
        scratch=[
            pltpu.VMEM((tokens, width), BF16), pltpu.VMEM((1, tokens), F32),
            pltpu.SemaphoreType.DMA((2,)),
        ],
    )
    send_rows, got_grad = lax.optimization_barrier((send_rows, got_grad))
    send_rows = send_rows.reshape(sp_count, padded, half)
    got_rows = lax.all_to_all(send_rows, "sp", 0, 0, tiled=True)
    ends = jnp.sum(got_rows[:, padded - 1, :3].astype(F32), axis=1)
    rows_own = got_rows.reshape(slots, half)
    running = jnp.cumsum(log_decay[:, 0])
    last = running[-1]

    grad_own = lax.all_gather(got_grad, "y", axis=1, tiled=True)
    rows_own, grad_own = lax.optimization_barrier((rows_own, grad_own))
    (part,) = call(
        own_body,
        [("v", rows_own), ("v", grad_own), ("h", mine), ("v", cross)],
        [((slots, 6 * units), SWAP_TYPE)],
        scratch=[
            pltpu.VMEM(mine.shape, BF16), pltpu.SemaphoreType.DMA((2,)),
        ],
        flops=12 * slots * half * units,
    )
    pair = lax.ppermute(part, "c", SWAP)
    act, both, pieces = call(
        units_body,
        [("v", part), ("v", pair), ("h", mine), ("v", cross)],
        [
            ((short, 2 * units), BF16, "h"), ((slots, 4 * units), BF16, "h"),
            ((8, slots, chunk), BF16, "h"),
        ],
        scratch=[
            pltpu.VMEM((2, 8, chunk, units), BF16), pltpu.VMEM((short, 2 * units), BF16), pltpu.VMEM((slots, 4 * units), BF16),
            pltpu.VMEM((8, slots, chunk), BF16),
            pltpu.SemaphoreType.DMA((1,)), pltpu.SemaphoreType.DMA((10,)),
        ],
        flops=8 * slots * half * units,
    )
    pieces = lax.all_to_all(pieces, "y", 0, 0, tiled=True)

    w_parts = dot(rows_own, both, ALONG).astype(BF16)
    w_own = w_parts[:, : 2 * units]
    w_other = lax.ppermute(w_parts[:, 2 * units :], "c", SWAP)
    w_grads = joined_rows(w_own, w_other, core)
    gate_w_grad, up_w_grad = w_grads[:, :units], w_grads[:, units:]
    down_parts = dot(act, grad_own, ALONG).astype(BF16)
    down_other = lax.ppermute(down_parts[units:], "c", SWAP)
    down_grad = joined_columns(down_parts[:units], down_other, core)

    (share,) = call(sum_body, [("v", pieces)], [((slots, chunk), BF16)])
    returned = lax.all_to_all(
        share.reshape(sp_count, padded, chunk), "sp", 0, 0, tiled=True
    ).reshape(slots, chunk)
    stream_part = (out_grad.astype(F32) + dot(picker, returned)).astype(BF16)
    stream = lax.all_gather(stream_part, TP, axis=1, tiled=True)

    rising = jnp.exp(running)[:, None]
    rows = 40
    ret_grad, payload = call(
        pack_body,
        [("v", stream), ("v", out_proj), ("v", retained), ("v", queries.T), ("v", rising.T.astype(BF16))],
        [((tokens, value_dim), BF16), ((sp_count, value_dim // 2 + rows, 128), BF16)],
        flops=4 * tokens * width * value_dim,
    )
    got = lax.all_to_all(payload, "sp", 0, 0, tiled=True)

    order = jnp.arange(sp_count)
    between = (order[None, :] > block) & (order[None, :] < order[:, None])
    factors = jnp.where(
        order > block, jnp.exp(jnp.sum(jnp.where(between, ends[None, :], 0.0), axis=1)), 0.0
    )
    q, k, v, o = (a.astype(F32) for a in (queries, keys, values, ret_grad))
    place = jnp.arange(tokens)
    causal = place[:, None] >= place[None, :]
    diff = running[:, None] - running[None, :]
    decay = jnp.where(causal, jnp.exp(jnp.minimum(diff, 0.0)), 0.0)
    scores = dot(q, k, ACROSS) * decay
    prob_grad = dot(o, v, ACROSS) * decay
    tail = jnp.exp(last - running)[:, None]
    query_grad = dot(prob_grad, k) + rising * dot(o, incoming_state[0, 0], ACROSS)
    key_part = dot(q, prob_grad, ALONG)
    value_part = dot(scores, o, ALONG)
    key_grad, value_grad, out_proj_grad = call(
        last_body,
        [
            ("s", factors), ("v", got), ("v", keys), ("v", values), ("v", tail),
            ("v", tail.T), ("v", key_part), ("v", value_part),
        ],
        [
            ((key_dim, tokens), BF16), ((tokens, value_dim), BF16),
            ((width // sp_count, value_dim), F32),
        ],
    )
    return (
        gate_w_grad[None],
        up_w_grad[None],
        down_grad[None],
        out_proj_grad,
        query_grad.astype(BF16),
        key_grad.T,
        value_grad,
    )


def solution(mesh):
    torus = Mesh(mesh.devices.reshape(mesh.shape["sp"], 8, 2), ("sp", "y", "c"))
    placed = (
        P("sp", None),
        P("sp", TP),
        P("sp", None),
        P("sp", None),
        P("sp", None, TP),
        P("sp", None, TP),
        P("sp", TP, None),
        P(TP, None),
        P("sp", TP),
        P("sp", TP),
        P("sp", TP),
        P("sp", TP),
        P("sp", TP),
        P("sp", TP, None, None),
    )
    return jax.shard_map(
        on_device,
        mesh=torus,
        in_specs=placed,
        out_specs=(
            P("sp", None, TP),
            P("sp", None, TP),
            P("sp", TP, None),
            P("sp", TP),
            P("sp", TP),
            P("sp", TP),
            P("sp", TP),
        ),
        check_vma=False,
    )
```

```python
import functools

import jax
import jax.numpy as jnp
from jax import lax
from jax.experimental import pallas as pl
from jax.experimental.pallas import tpu as pltpu
from jax.sharding import Mesh
from jax.sharding import PartitionSpec as P

TP = ("y", "c")
F32 = jnp.float32
BF16 = jnp.bfloat16
PLAIN = (((1,), (0,)), ((), ()))
ACROSS = (((1,), (1,)), ((), ()))
ALONG = (((0,), (0,)), ((), ()))
SWAP = [(0, 1), (1, 0)]
SWAP_TYPE = BF16
VMEM = pl.BlockSpec(memory_space=pltpu.VMEM)
SMEM = pl.BlockSpec(memory_space=pltpu.SMEM)
HBM = pl.BlockSpec(memory_space=pltpu.HBM)
PLACES = {"s": SMEM, "v": VMEM, "h": HBM}


def dot(a, b, dims=PLAIN):
    return lax.dot_general(a, b, dims, preferred_element_type=F32)


def call(body, ins, outs, scratch=(), flops=0, limit=20):
    specs = [PLACES[k] for k, _ in ins]
    places = tuple(PLACES[out[2] if len(out) > 2 else "v"] for out in outs)
    arrays = [
        pltpu.with_memory_space_constraint(a, pltpu.HBM) if k == "h" else a for k, a in ins
    ]
    return pl.pallas_call(
        body,
        in_specs=specs,
        out_specs=places,
        out_shape=tuple(
            pltpu.HBM(out[0], out[1]) if len(out) > 2 else jax.ShapeDtypeStruct(out[0], out[1])
            for out in outs
        ),
        scratch_shapes=list(scratch),
        compiler_params=pltpu.CompilerParams(vmem_limit_bytes=limit << 20),
        cost_estimate=pl.CostEstimate(flops=flops, transcendentals=0, bytes_accessed=0),
    )(*arrays)


def in_three(x):
    high = x.astype(BF16)
    rest = x - high.astype(F32)
    middle = rest.astype(BF16)
    low = (rest - middle.astype(F32)).astype(BF16)
    return high, middle, low


def started(pairs, sems):
    copies = [
        pltpu.make_async_copy(source, target, sems.at[k])
        for k, (source, target) in enumerate(pairs)
    ]
    for copy in copies:
        copy.start()
    return copies


def waited(copies):
    for copy in copies:
        copy.wait()


def setup_body(
    ids_hbm, weight_hbm, grad_hbm, picker_ref, send_ref, ids_ref, weight_ref, grad_ref, sems,
    *, experts, padded,
):
    waited(
        started([(ids_hbm, ids_ref), (weight_hbm, weight_ref), (grad_hbm, grad_ref)], sems)
    )
    tokens = ids_ref.shape[1]
    slots = experts * padded
    grad = grad_ref[...].astype(F32)
    row = lax.broadcasted_iota(jnp.int32, (tokens, tokens), 0)
    col = lax.broadcasted_iota(jnp.int32, (tokens, tokens), 1)
    same = jnp.where(row == col, 1.0, 0.0).astype(BF16)
    earlier = jnp.where(row > col, 1.0, 0.0).astype(BF16)
    lines = jnp.concatenate(
        [ids_ref[...].astype(F32)] + [p.astype(F32) for p in in_three(weight_ref[...])], axis=0
    )
    columns = dot(same, lines.astype(BF16), ACROSS)
    ids = columns[:, :2]
    names = lax.broadcasted_iota(jnp.int32, (tokens, experts), 1).astype(F32)
    onehot = [jnp.where(ids[:, j : j + 1] == names, 1.0, 0.0) for j in (0, 1)]
    before = dot(earlier, (onehot[0] + onehot[1]).astype(BF16))
    spots = lax.broadcasted_iota(jnp.int32, (tokens, slots), 1)
    picker, sent = None, None
    for j in (0, 1):
        rank = jnp.sum(before * onehot[j], axis=1, keepdims=True)
        slot = (ids[:, j : j + 1] * padded + rank).astype(jnp.int32)
        hits = jnp.where(spots == slot, 1.0, 0.0).astype(BF16)
        high, middle, low = (columns[:, k + j : k + j + 1] for k in (2, 4, 6))
        weight = (high + middle) + low
        part = dot(hits, (grad * weight).astype(BF16), ALONG)
        picker = hits if picker is None else picker + hits
        sent = part if sent is None else sent + part
    picker_ref[...] = picker
    send_ref[...] = sent.astype(BF16)


def rows_body(
    core_ref, picker_ref, input_hbm, decay_hbm, send_ref, input_ref, decay_ref, sems, *, padded
):
    waited(started([(input_hbm, input_ref), (decay_hbm, decay_ref)], sems))
    rows = dot(picker_ref[...], half_columns(input_ref, core_ref[0]), ALONG)
    parts = in_three(jnp.sum(decay_ref[...], axis=1, keepdims=True))
    lane = lax.broadcasted_iota(jnp.int32, rows.shape, 1)
    row = lax.broadcasted_iota(jnp.int32, rows.shape, 0)
    extra = jnp.zeros((1, 1), F32)
    for k, part in enumerate(parts):
        extra = jnp.where(lane == k, part.astype(F32), extra)
    send_ref[...] = jnp.where((row & (padded - 1)) == padded - 1, extra, rows).astype(BF16)


def half_columns(ref, core):
    chunk = 128
    pieces = [
        ref[:, pl.ds(pl.multiple_of((2 * k + core) * chunk, chunk), chunk)]
        for k in range(ref.shape[1] // (2 * chunk))
    ]
    return jnp.concatenate(pieces, axis=1)


def prep_body(
    core_ref, gate_hbm, up_hbm, down_hbm, mine_hbm, theirs_hbm, mine_ref, theirs_ref, sems, out_sems
):
    core = core_ref[0]
    count, chunk = gate_hbm.shape[0], gate_hbm.shape[2]
    pairs = []
    for target, half in ((theirs_ref, 1 - core), (mine_ref, core)):
        pairs += [(gate_hbm.at[:, half], target.at[0]), (up_hbm.at[:, half], target.at[1])]
        for k in range(count):
            at = pl.multiple_of((2 * k + half) * chunk, chunk)
            pairs.append((down_hbm.at[:, pl.ds(at, chunk)], target.at[2, k]))
    waited(started(pairs, sems))
    waited(started([(theirs_ref, theirs_hbm), (mine_ref, mine_hbm)], out_sems))


def side_by_side(refs):
    parts = [ref[k] for ref in refs for k in (0, 1)]
    return jnp.concatenate([p.reshape(-1, p.shape[2]) for p in parts], axis=1)


def lined_up(ref):
    return jnp.concatenate([ref[2, k] for k in range(ref.shape[1])], axis=1)


def own_body(rows_ref, grad_ref, mine_hbm, cross_ref, out_ref, mine_ref, sems):
    units = mine_ref.shape[3]
    short = grad_ref.shape[0]
    copies = started(
        [(mine_hbm.at[part], mine_ref.at[part]) for part in (pl.ds(2, 1), pl.ds(0, 2))], sems
    )
    crossed = dot(rows_ref[...], side_by_side((cross_ref,))).astype(out_ref.dtype)
    out_ref[:, 3 * units : 5 * units] = crossed
    waited(copies[:1])
    downs = jnp.concatenate([lined_up(mine_ref), lined_up(cross_ref)], axis=0)
    back = dot(grad_ref[...], downs, ACROSS).astype(out_ref.dtype)
    blank = jnp.zeros((8, units), out_ref.dtype)
    for k in (0, 1):
        at = 3 * units * k + 2 * units
        out_ref[pl.ds(out_ref.shape[0] - 8, 8), at : at + units] = blank
        out_ref[pl.ds(0, short), at : at + units] = back[:, units * k : units * (k + 1)]
    waited(copies[1:])
    out_ref[:, : 2 * units] = dot(rows_ref[...], side_by_side((mine_ref,))).astype(out_ref.dtype)


def units_body(
    part_ref, pair_ref, mine_hbm, cross_ref, act_hbm, both_hbm, out_hbm,
    mine_ref, act_ref, both_ref, out_ref, sems, out_sems,
):
    units = mine_ref.shape[3]
    chunk = mine_ref.shape[2]
    short = act_ref.shape[0]
    copies = started([(mine_hbm.at[pl.ds(0, 2)], mine_ref)], sems)
    for k in (0, 1):
        at, there = 3 * units * k, 3 * units * (1 - k)
        gate, up, act_grad = (
            part_ref[:, at + j * units : at + (j + 1) * units].astype(F32)
            + pair_ref[:, there + j * units : there + (j + 1) * units].astype(F32)
            for j in range(3)
        )
        sig = jax.nn.sigmoid(gate)
        swish = gate * sig
        act_ref[:, k * units : (k + 1) * units] = (swish * up).astype(BF16)[:short]
        both_ref[:, 2 * k * units : (2 * k + 1) * units] = (
            act_grad * up * sig * (1.0 + gate * (1.0 - sig))
        ).astype(BF16)
        both_ref[:, (2 * k + 1) * units : (2 * k + 2) * units] = (act_grad * swish).astype(BF16)
    count = out_ref.shape[0]
    sent = []
    for k, (source, target) in enumerate([(act_ref, act_hbm), (both_ref, both_hbm)]):
        copy = pltpu.make_async_copy(source, target, out_sems.at[count + k])
        copy.start()
        sent.append(copy)
    waited(copies)
    grads = both_ref[...]
    for k in range(0, count, 2):
        two = jnp.concatenate(
            [
                ref[j, pl.ds(k, 2)].reshape(2 * chunk, units)
                for ref in (mine_ref, cross_ref)
                for j in (0, 1)
            ],
            axis=1,
        )
        part = dot(grads, two, ACROSS).astype(BF16)
        for j in (0, 1):
            piece = part[:, chunk * j : chunk * (j + 1)]
            out_ref[k + j] = piece.reshape(out_ref.shape[1:])
            copy = pltpu.make_async_copy(out_ref.at[k + j], out_hbm.at[:, k + j], out_sems.at[k + j])
            copy.start()
            sent.append(copy)
    waited(sent)


def sum_body(parts_ref, out_ref):
    total = parts_ref[:, 0].astype(F32)
    for k in range(1, parts_ref.shape[1]):
        total = total + parts_ref[:, k].astype(F32)
    out_ref[...] = total.astype(BF16)


def pack_body(stream_ref, proj_ref, kept_ref, query_ref, rising_ref, ret_ref, pay_ref):
    stream = stream_ref[...]
    ret = dot(stream, proj_ref[...], ACROSS).astype(BF16)
    ret_ref[...] = ret
    inject = dot(query_ref[...] * rising_ref[...], ret)
    proj = dot(kept_ref[...], stream, ALONG)
    lanes = pay_ref.shape[2]
    width = proj.shape[0]
    fold = lanes - width
    rows = pay_ref.shape[1] - width // 2
    rest = inject.shape[0] - rows
    side = [inject[rows:, k * fold : (k + 1) * fold] for k in range(width // fold)]
    blank = jnp.zeros((rows - rest * len(side), fold), F32)
    top = jnp.concatenate(
        [inject[:rows], jnp.concatenate(side + [blank], axis=0)], axis=1
    ).astype(BF16)
    low = lax.broadcasted_iota(jnp.int32, (width // 2, lanes), 1) < lanes // 2
    for j in range(proj.shape[1] // lanes):
        tile = proj[:, j * lanes : (j + 1) * lanes]
        upper, under = tile[: width // 2], tile[width // 2 :]
        turned = [pltpu.roll(t, lanes // 2, 1) for t in (upper, under)]
        pay_ref[2 * j, :rows] = top
        pay_ref[2 * j, rows:] = jnp.where(low, upper, turned[1]).astype(BF16)
        pay_ref[2 * j + 1, :rows] = top
        pay_ref[2 * j + 1, rows:] = jnp.where(low, turned[0], under).astype(BF16)


def last_body(
    factor_ref, got_ref, keys_ref, values_ref, tail_ref, tail_row_ref, key_part_ref,
    value_part_ref, key_ref, value_ref, proj_ref,
):
    count, _, lanes = got_ref.shape
    key_dim, width = keys_ref.shape[1], values_ref.shape[1]
    rows = got_ref.shape[1] - width // 2
    fold = lanes - width
    rest = key_dim - rows
    state, total = None, None
    for m in range(count):
        part = got_ref[m, rows:].astype(F32)
        total = part if total is None else total + part
        scaled = factor_ref[m] * got_ref[m, :rows].astype(F32)
        state = scaled if state is None else state + scaled
    state = jnp.concatenate(
        [
            state[:, :width],
            jnp.concatenate(
                [state[k * rest : (k + 1) * rest, width:] for k in range(width // fold)], axis=1
            ),
        ],
        axis=0,
    ).astype(BF16)
    half = lanes // 2
    proj_ref[...] = jnp.concatenate([total[:, :half], total[:, half:]], axis=0).T
    tail = tail_ref[...]
    across = dot(state, values_ref[...], ACROSS)
    key_ref[...] = (key_part_ref[...] + tail_row_ref[...] * across).astype(BF16)
    value_ref[...] = (value_part_ref[...] + tail * dot(keys_ref[...], state)).astype(BF16)


def joined_rows(own, other, core):
    rows, cols = own.shape
    own, other = (a.reshape(8, 1, rows // 8, cols) for a in (own, other))
    first = jnp.where(core == 0, own, other)
    second = jnp.where(core == 0, other, own)
    return jnp.concatenate([first, second], axis=1).reshape(2 * rows, cols)


def joined_columns(own, other, core):
    rows, cols = own.shape
    own, other = (a.reshape(rows, 8, 1, cols // 8) for a in (own, other))
    first = jnp.where(core == 0, own, other)
    second = jnp.where(core == 0, other, own)
    return jnp.concatenate([first, second], axis=2).reshape(rows, 2 * cols)


def on_device(
    moe_input,
    out_grad,
    expert_ids,
    expert_weights,
    w_gate,
    w_up,
    w_down,
    out_proj,
    retained,
    queries,
    keys,
    values,
    log_decay,
    incoming_state,
):
    tokens, width = moe_input.shape
    sp_count = lax.axis_size("sp")
    padded = 16
    slots = sp_count * padded
    short = slots - 1
    core = lax.axis_index("c")
    block = lax.axis_index("sp")
    chunk = out_grad.shape[1]
    half = width // 2
    units = w_gate.shape[2]
    key_dim, value_dim = queries.shape[1], values.shape[1]

    core_1 = core.astype(jnp.int32).reshape(1)
    picker, send_grad = call(
        functools.partial(setup_body, experts=sp_count, padded=padded),
        [("h", expert_ids.T), ("h", expert_weights.T), ("h", out_grad)],
        [((tokens, slots), BF16), ((slots, chunk), BF16)],
        scratch=[
            pltpu.VMEM((2, tokens), jnp.int32), pltpu.VMEM((2, tokens), F32),
            pltpu.VMEM((tokens, chunk), BF16), pltpu.SemaphoreType.DMA((3,)),
        ],
    )
    gate_4 = w_gate.reshape(8, 2, chunk, units)
    up_4 = w_up.reshape(8, 2, chunk, units)
    down_2 = w_down[0]
    halves = [((3, 8, chunk, units), BF16, "h")] * 2
    mine, theirs = call(
        prep_body,
        [("s", core_1), ("h", gate_4), ("h", up_4), ("h", down_2)],
        halves,
        scratch=[
            pltpu.VMEM((3, 8, chunk, units), BF16), pltpu.VMEM((3, 8, chunk, units), BF16),
            pltpu.SemaphoreType.DMA((20,)), pltpu.SemaphoreType.DMA((2,)),
        ],
    )
    cross = lax.ppermute(theirs, "c", SWAP)
    got_grad = lax.all_to_all(send_grad.reshape(sp_count, padded, chunk), "sp", 0, 0, tiled=True)
    got_grad = got_grad.reshape(slots, chunk)[:short]

    (send_rows,) = call(
        functools.partial(rows_body, padded=padded),
        [("s", core_1), ("v", picker), ("h", moe_input), ("h", log_decay.T)],
        [((slots, half), BF16)],
        scratch=[
            pltpu.VMEM((tokens, width), BF16), pltpu.VMEM((1, tokens), F32),
            pltpu.SemaphoreType.DMA((2,)),
        ],
    )
    send_rows, got_grad = lax.optimization_barrier((send_rows, got_grad))
    send_rows = send_rows.reshape(sp_count, padded, half)
    got_rows = lax.all_to_all(send_rows, "sp", 0, 0, tiled=True)
    ends = jnp.sum(got_rows[:, padded - 1, :3].astype(F32), axis=1)
    rows_own = got_rows.reshape(slots, half)
    running = jnp.cumsum(log_decay[:, 0])
    last = running[-1]

    grad_own = lax.all_gather(got_grad, "y", axis=1, tiled=True)
    rows_own, grad_own = lax.optimization_barrier((rows_own, grad_own))
    (part,) = call(
        own_body,
        [("v", rows_own), ("v", grad_own), ("h", mine), ("v", cross)],
        [((slots, 6 * units), SWAP_TYPE)],
        scratch=[
            pltpu.VMEM(mine.shape, BF16), pltpu.SemaphoreType.DMA((2,)),
        ],
        flops=12 * slots * half * units,
    )
    pair = lax.ppermute(part, "c", SWAP)
    act, both, pieces = call(
        units_body,
        [("v", part), ("v", pair), ("h", mine), ("v", cross)],
        [
            ((short, 2 * units), BF16, "h"), ((slots, 4 * units), BF16, "h"),
            ((sp_count, 8, padded, chunk), BF16, "h"),
        ],
        scratch=[
            pltpu.VMEM((2, 8, chunk, units), BF16), pltpu.VMEM((short, 2 * units), BF16), pltpu.VMEM((slots, 4 * units), BF16),
            pltpu.VMEM((8, sp_count, padded, chunk), BF16),
            pltpu.SemaphoreType.DMA((1,)), pltpu.SemaphoreType.DMA((10,)),
        ],
        flops=8 * slots * half * units,
    )
    pieces = pieces.reshape(sp_count * 8, padded, chunk)
    pieces = lax.all_to_all(pieces, ("sp", "y"), 0, 0, tiled=True)
    pieces = pieces.reshape(sp_count, 8, padded, chunk)

    w_parts = dot(rows_own, both, ALONG).astype(BF16)
    w_own = w_parts[:, : 2 * units]
    w_other = lax.ppermute(w_parts[:, 2 * units :], "c", SWAP)
    w_grads = joined_rows(w_own, w_other, core)
    gate_w_grad, up_w_grad = w_grads[:, :units], w_grads[:, units:]
    down_parts = dot(act, grad_own, ALONG).astype(BF16)
    down_other = lax.ppermute(down_parts[units:], "c", SWAP)
    down_grad = joined_columns(down_parts[:units], down_other, core)

    (returned,) = call(sum_body, [("v", pieces)], [((sp_count, padded, chunk), BF16)])
    returned = returned.reshape(slots, chunk)
    stream_part = (out_grad.astype(F32) + dot(picker, returned)).astype(BF16)
    stream = lax.all_gather(stream_part, TP, axis=1, tiled=True)

    rising = jnp.exp(running)[:, None]
    rows = 40
    ret_grad, payload = call(
        pack_body,
        [("v", stream), ("v", out_proj), ("v", retained), ("v", queries.T), ("v", rising.T.astype(BF16))],
        [((tokens, value_dim), BF16), ((sp_count, value_dim // 2 + rows, 128), BF16)],
        flops=4 * tokens * width * value_dim,
    )
    got = lax.all_to_all(payload, "sp", 0, 0, tiled=True)

    order = jnp.arange(sp_count)
    between = (order[None, :] > block) & (order[None, :] < order[:, None])
    factors = jnp.where(
        order > block, jnp.exp(jnp.sum(jnp.where(between, ends[None, :], 0.0), axis=1)), 0.0
    )
    q, k, v, o = (a.astype(F32) for a in (queries, keys, values, ret_grad))
    place = jnp.arange(tokens)
    causal = place[:, None] >= place[None, :]
    diff = running[:, None] - running[None, :]
    decay = jnp.where(causal, jnp.exp(jnp.minimum(diff, 0.0)), 0.0)
    scores = dot(q, k, ACROSS) * decay
    prob_grad = dot(o, v, ACROSS) * decay
    tail = jnp.exp(last - running)[:, None]
    query_grad = dot(prob_grad, k) + rising * dot(o, incoming_state[0, 0], ACROSS)
    key_part = dot(q, prob_grad, ALONG)
    value_part = dot(scores, o, ALONG)
    key_grad, value_grad, out_proj_grad = call(
        last_body,
        [
            ("s", factors), ("v", got), ("v", keys), ("v", values), ("v", tail),
            ("v", tail.T), ("v", key_part), ("v", value_part),
        ],
        [
            ((key_dim, tokens), BF16), ((tokens, value_dim), BF16),
            ((width // sp_count, value_dim), F32),
        ],
    )
    return (
        gate_w_grad[None],
        up_w_grad[None],
        down_grad[None],
        out_proj_grad,
        query_grad.astype(BF16),
        key_grad.T,
        value_grad,
    )


def solution(mesh):
    torus = Mesh(mesh.devices.reshape(mesh.shape["sp"], 8, 2), ("sp", "y", "c"))
    placed = (
        P("sp", None),
        P("sp", TP),
        P("sp", None),
        P("sp", None),
        P("sp", None, TP),
        P("sp", None, TP),
        P("sp", TP, None),
        P(TP, None),
        P("sp", TP),
        P("sp", TP),
        P("sp", TP),
        P("sp", TP),
        P("sp", TP),
        P("sp", TP, None, None),
    )
    return jax.shard_map(
        on_device,
        mesh=torus,
        in_specs=placed,
        out_specs=(
            P("sp", None, TP),
            P("sp", None, TP),
            P("sp", TP, None),
            P("sp", TP),
            P("sp", TP),
            P("sp", TP),
            P("sp", TP),
        ),
        check_vma=False,
    )
```

```python
import functools

import jax
import jax.numpy as jnp
from jax import lax
from jax.experimental import pallas as pl
from jax.experimental.pallas import tpu as pltpu
from jax.sharding import Mesh
from jax.sharding import PartitionSpec as P

TP = ("y", "c")
F32 = jnp.float32
BF16 = jnp.bfloat16
PLAIN = (((1,), (0,)), ((), ()))
ACROSS = (((1,), (1,)), ((), ()))
ALONG = (((0,), (0,)), ((), ()))
SWAP = [(0, 1), (1, 0)]
SWAP_TYPE = BF16
VMEM = pl.BlockSpec(memory_space=pltpu.VMEM)
SMEM = pl.BlockSpec(memory_space=pltpu.SMEM)
HBM = pl.BlockSpec(memory_space=pltpu.HBM)
PLACES = {"s": SMEM, "v": VMEM, "h": HBM}


def dot(a, b, dims=PLAIN):
    return lax.dot_general(a, b, dims, preferred_element_type=F32)


def call(body, ins, outs, scratch=(), flops=0, limit=20):
    specs = [PLACES[k] for k, _ in ins]
    places = tuple(PLACES[out[2] if len(out) > 2 else "v"] for out in outs)
    arrays = [
        pltpu.with_memory_space_constraint(a, pltpu.HBM) if k == "h" else a for k, a in ins
    ]
    return pl.pallas_call(
        body,
        in_specs=specs,
        out_specs=places,
        out_shape=tuple(
            pltpu.HBM(out[0], out[1]) if len(out) > 2 else jax.ShapeDtypeStruct(out[0], out[1])
            for out in outs
        ),
        scratch_shapes=list(scratch),
        compiler_params=pltpu.CompilerParams(vmem_limit_bytes=limit << 20),
        cost_estimate=pl.CostEstimate(flops=flops, transcendentals=0, bytes_accessed=0),
    )(*arrays)


def in_three(x):
    high = x.astype(BF16)
    rest = x - high.astype(F32)
    middle = rest.astype(BF16)
    low = (rest - middle.astype(F32)).astype(BF16)
    return high, middle, low


def started(pairs, sems):
    copies = [
        pltpu.make_async_copy(source, target, sems.at[k])
        for k, (source, target) in enumerate(pairs)
    ]
    for copy in copies:
        copy.start()
    return copies


def waited(copies):
    for copy in copies:
        copy.wait()


def setup_body(
    ids_hbm, weight_hbm, grad_hbm, picker_ref, send_ref, ids_ref, weight_ref, grad_ref, sems,
    *, experts, padded,
):
    waited(
        started([(ids_hbm, ids_ref), (weight_hbm, weight_ref), (grad_hbm, grad_ref)], sems)
    )
    tokens = ids_ref.shape[1]
    slots = experts * padded
    grad = grad_ref[...].astype(F32)
    row = lax.broadcasted_iota(jnp.int32, (tokens, tokens), 0)
    col = lax.broadcasted_iota(jnp.int32, (tokens, tokens), 1)
    same = jnp.where(row == col, 1.0, 0.0).astype(BF16)
    earlier = jnp.where(row > col, 1.0, 0.0).astype(BF16)
    lines = jnp.concatenate(
        [ids_ref[...].astype(F32)] + [p.astype(F32) for p in in_three(weight_ref[...])], axis=0
    )
    columns = dot(same, lines.astype(BF16), ACROSS)
    ids = columns[:, :2]
    names = lax.broadcasted_iota(jnp.int32, (tokens, experts), 1).astype(F32)
    onehot = [jnp.where(ids[:, j : j + 1] == names, 1.0, 0.0) for j in (0, 1)]
    before = dot(earlier, (onehot[0] + onehot[1]).astype(BF16))
    spots = lax.broadcasted_iota(jnp.int32, (tokens, slots), 1)
    picker, sent = None, None
    for j in (0, 1):
        rank = jnp.sum(before * onehot[j], axis=1, keepdims=True)
        slot = (ids[:, j : j + 1] * padded + rank).astype(jnp.int32)
        hits = jnp.where(spots == slot, 1.0, 0.0).astype(BF16)
        high, middle, low = (columns[:, k + j : k + j + 1] for k in (2, 4, 6))
        weight = (high + middle) + low
        part = dot(hits, (grad * weight).astype(BF16), ALONG)
        picker = hits if picker is None else picker + hits
        sent = part if sent is None else sent + part
    picker_ref[...] = picker
    send_ref[...] = sent.astype(BF16)


def rows_body(
    core_ref, picker_ref, input_hbm, decay_hbm, send_ref, input_ref, decay_ref, sems, *, padded
):
    waited(started([(input_hbm, input_ref), (decay_hbm, decay_ref)], sems))
    rows = dot(picker_ref[...], half_columns(input_ref, core_ref[0]), ALONG)
    parts = in_three(jnp.sum(decay_ref[...], axis=1, keepdims=True))
    lane = lax.broadcasted_iota(jnp.int32, rows.shape, 1)
    row = lax.broadcasted_iota(jnp.int32, rows.shape, 0)
    extra = jnp.zeros((1, 1), F32)
    for k, part in enumerate(parts):
        extra = jnp.where(lane == k, part.astype(F32), extra)
    send_ref[...] = jnp.where((row & (padded - 1)) == padded - 1, extra, rows).astype(BF16)


def half_columns(ref, core):
    chunk = 128
    pieces = [
        ref[:, pl.ds(pl.multiple_of((2 * k + core) * chunk, chunk), chunk)]
        for k in range(ref.shape[1] // (2 * chunk))
    ]
    return jnp.concatenate(pieces, axis=1)


def prep_body(
    core_ref, gate_hbm, up_hbm, down_hbm, mine_hbm, theirs_hbm, mine_ref, theirs_ref, sems, out_sems
):
    core = core_ref[0]
    count, chunk = gate_hbm.shape[0], gate_hbm.shape[2]
    pairs = []
    for target, half in ((theirs_ref, 1 - core), (mine_ref, core)):
        pairs += [(gate_hbm.at[:, half], target.at[0]), (up_hbm.at[:, half], target.at[1])]
        for k in range(count):
            at = pl.multiple_of((2 * k + half) * chunk, chunk)
            pairs.append((down_hbm.at[:, pl.ds(at, chunk)], target.at[2, k]))
    waited(started(pairs, sems))
    waited(started([(theirs_ref, theirs_hbm), (mine_ref, mine_hbm)], out_sems))


def side_by_side(refs):
    parts = [ref[k] for ref in refs for k in (0, 1)]
    return jnp.concatenate([p.reshape(-1, p.shape[2]) for p in parts], axis=1)


def lined_up(ref):
    return jnp.concatenate([ref[2, k] for k in range(ref.shape[1])], axis=1)


def own_body(rows_hbm, grad_ref, mine_hbm, cross_ref, out_ref, mine_ref, rows_ref, sems):
    units = mine_ref.shape[3]
    short = grad_ref.shape[0]
    parts = [(mine_hbm.at[part], mine_ref.at[part]) for part in (pl.ds(2, 1), pl.ds(0, 2))]
    copies = started([parts[0], (rows_hbm, rows_ref), parts[1]], sems)
    waited(copies[:1])
    downs = jnp.concatenate([lined_up(mine_ref), lined_up(cross_ref)], axis=0)
    back = dot(grad_ref[...], downs, ACROSS).astype(out_ref.dtype)
    blank = jnp.zeros((8, units), out_ref.dtype)
    for k in (0, 1):
        at = 3 * units * k + 2 * units
        out_ref[pl.ds(out_ref.shape[0] - 8, 8), at : at + units] = blank
        out_ref[pl.ds(0, short), at : at + units] = back[:, units * k : units * (k + 1)]
    waited(copies[1:2])
    crossed = dot(rows_ref[...], side_by_side((cross_ref,))).astype(out_ref.dtype)
    out_ref[:, 3 * units : 5 * units] = crossed
    waited(copies[2:])
    out_ref[:, : 2 * units] = dot(rows_ref[...], side_by_side((mine_ref,))).astype(out_ref.dtype)


def units_body(
    part_ref, pair_ref, mine_hbm, cross_ref, act_hbm, both_hbm, out_hbm,
    mine_ref, act_ref, both_ref, out_ref, sems, out_sems,
):
    units = mine_ref.shape[3]
    chunk = mine_ref.shape[2]
    short = act_ref.shape[0]
    copies = started([(mine_hbm.at[pl.ds(0, 2)], mine_ref)], sems)
    for k in (0, 1):
        at, there = 3 * units * k, 3 * units * (1 - k)
        gate, up, act_grad = (
            part_ref[:, at + j * units : at + (j + 1) * units].astype(F32)
            + pair_ref[:, there + j * units : there + (j + 1) * units].astype(F32)
            for j in range(3)
        )
        sig = jax.nn.sigmoid(gate)
        swish = gate * sig
        act_ref[:, k * units : (k + 1) * units] = (swish * up).astype(BF16)[:short]
        both_ref[:, 2 * k * units : (2 * k + 1) * units] = (
            act_grad * up * sig * (1.0 + gate * (1.0 - sig))
        ).astype(BF16)
        both_ref[:, (2 * k + 1) * units : (2 * k + 2) * units] = (act_grad * swish).astype(BF16)
    count = out_ref.shape[0]
    sent = []
    for k, (source, target) in enumerate([(act_ref, act_hbm), (both_ref, both_hbm)]):
        copy = pltpu.make_async_copy(source, target, out_sems.at[count + k])
        copy.start()
        sent.append(copy)
    waited(copies)
    grads = both_ref[...]
    for k in range(0, count, 2):
        two = jnp.concatenate(
            [
                ref[j, pl.ds(k, 2)].reshape(2 * chunk, units)
                for ref in (mine_ref, cross_ref)
                for j in (0, 1)
            ],
            axis=1,
        )
        part = dot(grads, two, ACROSS).astype(BF16)
        for j in (0, 1):
            piece = part[:, chunk * j : chunk * (j + 1)]
            out_ref[k + j] = piece.reshape(out_ref.shape[1:])
            copy = pltpu.make_async_copy(out_ref.at[k + j], out_hbm.at[:, k + j], out_sems.at[k + j])
            copy.start()
            sent.append(copy)
    waited(sent)


def sum_body(parts_ref, out_ref):
    total = parts_ref[:, 0].astype(F32)
    for k in range(1, parts_ref.shape[1]):
        total = total + parts_ref[:, k].astype(F32)
    out_ref[...] = total.astype(BF16)


def pack_body(stream_ref, proj_ref, kept_ref, query_ref, rising_ref, ret_ref, pay_ref):
    stream = stream_ref[...]
    ret = dot(stream, proj_ref[...], ACROSS).astype(BF16)
    ret_ref[...] = ret
    inject = dot(query_ref[...] * rising_ref[...], ret)
    proj = dot(kept_ref[...], stream, ALONG)
    lanes = pay_ref.shape[2]
    width = proj.shape[0]
    fold = lanes - width
    rows = pay_ref.shape[1] - width // 2
    rest = inject.shape[0] - rows
    side = [inject[rows:, k * fold : (k + 1) * fold] for k in range(width // fold)]
    blank = jnp.zeros((rows - rest * len(side), fold), F32)
    top = jnp.concatenate(
        [inject[:rows], jnp.concatenate(side + [blank], axis=0)], axis=1
    ).astype(BF16)
    low = lax.broadcasted_iota(jnp.int32, (width // 2, lanes), 1) < lanes // 2
    for j in range(proj.shape[1] // lanes):
        tile = proj[:, j * lanes : (j + 1) * lanes]
        upper, under = tile[: width // 2], tile[width // 2 :]
        turned = [pltpu.roll(t, lanes // 2, 1) for t in (upper, under)]
        pay_ref[2 * j, :rows] = top
        pay_ref[2 * j, rows:] = jnp.where(low, upper, turned[1]).astype(BF16)
        pay_ref[2 * j + 1, :rows] = top
        pay_ref[2 * j + 1, rows:] = jnp.where(low, turned[0], under).astype(BF16)


def last_body(
    factor_ref, got_ref, keys_ref, values_ref, tail_ref, tail_row_ref, key_part_ref,
    value_part_ref, key_ref, value_ref, proj_ref,
):
    count, _, lanes = got_ref.shape
    key_dim, width = keys_ref.shape[1], values_ref.shape[1]
    rows = got_ref.shape[1] - width // 2
    fold = lanes - width
    rest = key_dim - rows
    state, total = None, None
    for m in range(count):
        part = got_ref[m, rows:].astype(F32)
        total = part if total is None else total + part
        scaled = factor_ref[m] * got_ref[m, :rows].astype(F32)
        state = scaled if state is None else state + scaled
    state = jnp.concatenate(
        [
            state[:, :width],
            jnp.concatenate(
                [state[k * rest : (k + 1) * rest, width:] for k in range(width // fold)], axis=1
            ),
        ],
        axis=0,
    ).astype(BF16)
    half = lanes // 2
    proj_ref[...] = jnp.concatenate([total[:, :half], total[:, half:]], axis=0).T
    tail = tail_ref[...]
    across = dot(state, values_ref[...], ACROSS)
    key_ref[...] = (key_part_ref[...] + tail_row_ref[...] * across).astype(BF16)
    value_ref[...] = (value_part_ref[...] + tail * dot(keys_ref[...], state)).astype(BF16)


def joined_rows(own, other, core):
    rows, cols = own.shape
    own, other = (a.reshape(8, 1, rows // 8, cols) for a in (own, other))
    first = jnp.where(core == 0, own, other)
    second = jnp.where(core == 0, other, own)
    return jnp.concatenate([first, second], axis=1).reshape(2 * rows, cols)


def joined_columns(own, other, core):
    rows, cols = own.shape
    own, other = (a.reshape(rows, 8, 1, cols // 8) for a in (own, other))
    first = jnp.where(core == 0, own, other)
    second = jnp.where(core == 0, other, own)
    return jnp.concatenate([first, second], axis=2).reshape(rows, 2 * cols)


def on_device(
    moe_input,
    out_grad,
    expert_ids,
    expert_weights,
    w_gate,
    w_up,
    w_down,
    out_proj,
    retained,
    queries,
    keys,
    values,
    log_decay,
    incoming_state,
):
    tokens, width = moe_input.shape
    sp_count = lax.axis_size("sp")
    padded = 16
    slots = sp_count * padded
    short = slots - 1
    core = lax.axis_index("c")
    block = lax.axis_index("sp")
    chunk = out_grad.shape[1]
    half = width // 2
    units = w_gate.shape[2]
    key_dim, value_dim = queries.shape[1], values.shape[1]

    core_1 = core.astype(jnp.int32).reshape(1)
    picker, send_grad = call(
        functools.partial(setup_body, experts=sp_count, padded=padded),
        [("h", expert_ids.T), ("h", expert_weights.T), ("h", out_grad)],
        [((tokens, slots), BF16), ((slots, chunk), BF16)],
        scratch=[
            pltpu.VMEM((2, tokens), jnp.int32), pltpu.VMEM((2, tokens), F32),
            pltpu.VMEM((tokens, chunk), BF16), pltpu.SemaphoreType.DMA((3,)),
        ],
    )
    gate_4 = w_gate.reshape(8, 2, chunk, units)
    up_4 = w_up.reshape(8, 2, chunk, units)
    down_2 = w_down[0]
    halves = [((3, 8, chunk, units), BF16, "h")] * 2
    mine, theirs = call(
        prep_body,
        [("s", core_1), ("h", gate_4), ("h", up_4), ("h", down_2)],
        halves,
        scratch=[
            pltpu.VMEM((3, 8, chunk, units), BF16), pltpu.VMEM((3, 8, chunk, units), BF16),
            pltpu.SemaphoreType.DMA((20,)), pltpu.SemaphoreType.DMA((2,)),
        ],
    )
    cross = lax.ppermute(theirs, "c", SWAP)
    got_grad = lax.all_to_all(send_grad.reshape(sp_count, padded, chunk), "sp", 0, 0, tiled=True)
    got_grad = got_grad.reshape(slots, chunk)[:short]

    (send_rows,) = call(
        functools.partial(rows_body, padded=padded),
        [("s", core_1), ("v", picker), ("h", moe_input), ("h", log_decay.T)],
        [((slots, half), BF16)],
        scratch=[
            pltpu.VMEM((tokens, width), BF16), pltpu.VMEM((1, tokens), F32),
            pltpu.SemaphoreType.DMA((2,)),
        ],
    )
    send_rows, got_grad = lax.optimization_barrier((send_rows, got_grad))
    send_rows = send_rows.reshape(sp_count, padded, half)
    got_rows = lax.all_to_all(send_rows, "sp", 0, 0, tiled=True)
    ends = jnp.sum(got_rows[:, padded - 1, :3].astype(F32), axis=1)
    rows_own = got_rows.reshape(slots, half)
    running = jnp.cumsum(log_decay[:, 0])
    last = running[-1]

    grad_own = lax.all_gather(got_grad, "y", axis=1, tiled=True)
    rows_own, grad_own = lax.optimization_barrier((rows_own, grad_own))
    (part,) = call(
        own_body,
        [("h", rows_own), ("v", grad_own), ("h", mine), ("v", cross)],
        [((slots, 6 * units), SWAP_TYPE)],
        scratch=[
            pltpu.VMEM(mine.shape, BF16), pltpu.VMEM((slots, half), BF16),
            pltpu.SemaphoreType.DMA((3,)),
        ],
        flops=12 * slots * half * units,
    )
    pair = lax.ppermute(part, "c", SWAP)
    act, both, pieces = call(
        units_body,
        [("v", part), ("v", pair), ("h", mine), ("v", cross)],
        [
            ((short, 2 * units), BF16, "h"), ((slots, 4 * units), BF16, "h"),
            ((sp_count, 8, padded, chunk), BF16, "h"),
        ],
        scratch=[
            pltpu.VMEM((2, 8, chunk, units), BF16), pltpu.VMEM((short, 2 * units), BF16), pltpu.VMEM((slots, 4 * units), BF16),
            pltpu.VMEM((8, sp_count, padded, chunk), BF16),
            pltpu.SemaphoreType.DMA((1,)), pltpu.SemaphoreType.DMA((10,)),
        ],
        flops=8 * slots * half * units,
    )
    pieces = pieces.reshape(sp_count * 8, padded, chunk)
    pieces = lax.all_to_all(pieces, ("sp", "y"), 0, 0, tiled=True)
    pieces = pieces.reshape(sp_count, 8, padded, chunk)

    w_parts = dot(rows_own, both, ALONG).astype(BF16)
    w_own = w_parts[:, : 2 * units]
    w_other = lax.ppermute(w_parts[:, 2 * units :], "c", SWAP)
    w_grads = joined_rows(w_own, w_other, core)
    gate_w_grad, up_w_grad = w_grads[:, :units], w_grads[:, units:]
    down_parts = dot(act, grad_own, ALONG).astype(BF16)
    down_other = lax.ppermute(down_parts[units:], "c", SWAP)
    down_grad = joined_columns(down_parts[:units], down_other, core)

    (returned,) = call(sum_body, [("v", pieces)], [((sp_count, padded, chunk), BF16)])
    returned = returned.reshape(slots, chunk)
    stream_part = (out_grad.astype(F32) + dot(picker, returned)).astype(BF16)
    stream = lax.all_gather(stream_part, TP, axis=1, tiled=True)

    rising = jnp.exp(running)[:, None]
    rows = 40
    ret_grad, payload = call(
        pack_body,
        [("v", stream), ("v", out_proj), ("v", retained), ("v", queries.T), ("v", rising.T.astype(BF16))],
        [((tokens, value_dim), BF16), ((sp_count, value_dim // 2 + rows, 128), BF16)],
        flops=4 * tokens * width * value_dim,
    )
    got = lax.all_to_all(payload, "sp", 0, 0, tiled=True)

    order = jnp.arange(sp_count)
    between = (order[None, :] > block) & (order[None, :] < order[:, None])
    factors = jnp.where(
        order > block, jnp.exp(jnp.sum(jnp.where(between, ends[None, :], 0.0), axis=1)), 0.0
    )
    q, k, v, o = (a.astype(F32) for a in (queries, keys, values, ret_grad))
    place = jnp.arange(tokens)
    causal = place[:, None] >= place[None, :]
    diff = running[:, None] - running[None, :]
    decay = jnp.where(causal, jnp.exp(jnp.minimum(diff, 0.0)), 0.0)
    scores = dot(q, k, ACROSS) * decay
    prob_grad = dot(o, v, ACROSS) * decay
    tail = jnp.exp(last - running)[:, None]
    query_grad = dot(prob_grad, k) + rising * dot(o, incoming_state[0, 0], ACROSS)
    key_part = dot(q, prob_grad, ALONG)
    value_part = dot(scores, o, ALONG)
    key_grad, value_grad, out_proj_grad = call(
        last_body,
        [
            ("s", factors), ("v", got), ("v", keys), ("v", values), ("v", tail),
            ("v", tail.T), ("v", key_part), ("v", value_part),
        ],
        [
            ((key_dim, tokens), BF16), ((tokens, value_dim), BF16),
            ((width // sp_count, value_dim), F32),
        ],
    )
    return (
        gate_w_grad[None],
        up_w_grad[None],
        down_grad[None],
        out_proj_grad,
        query_grad.astype(BF16),
        key_grad.T,
        value_grad,
    )


def solution(mesh):
    torus = Mesh(mesh.devices.reshape(mesh.shape["sp"], 8, 2), ("sp", "y", "c"))
    placed = (
        P("sp", None),
        P("sp", TP),
        P("sp", None),
        P("sp", None),
        P("sp", None, TP),
        P("sp", None, TP),
        P("sp", TP, None),
        P(TP, None),
        P("sp", TP),
        P("sp", TP),
        P("sp", TP),
        P("sp", TP),
        P("sp", TP),
        P("sp", TP, None, None),
    )
    return jax.shard_map(
        on_device,
        mesh=torus,
        in_specs=placed,
        out_specs=(
            P("sp", None, TP),
            P("sp", None, TP),
            P("sp", TP, None),
            P("sp", TP),
            P("sp", TP),
            P("sp", TP),
            P("sp", TP),
        ),
        check_vma=False,
    )
```
